32 devices in a mesh: grp: 2 (over x), ep: 8 (over z, y), tp: 2 (over core).
Axes of the slice: x: 2, y: 2, z: 4, core: 2. Of those that a mesh axis runs over, the one named last changes fastest.
Arguments:
- tokens: bfloat16 [8192, 2048], P(('grp', 'ep'), 'tp'), parts along dimension 0, may hold values from -6 to 6
- norm_gain: float32 [2048], replicated, may hold values from 0.1 to 1.9
- expert_ids: int32 [8192, 2], P(('grp', 'ep')), parts along dimension 0, may hold values from 0 to 7, all different within a row; in each aligned block of 512 rows (0 to 511, 512 to 1023, ...) at most 192 rows name the same one
- route_weights: float32 [8192, 2], P(('grp', 'ep')), parts along dimension 0, may hold values from 0.1 to 1
- gate_weight: bfloat16 [8, 2048, 512], P('ep', None, 'tp'), may hold values from -0.125 to 0.125
- up_weight: bfloat16 [8, 2048, 512], P('ep', None, 'tp'), may hold values from -0.125 to 0.125
- down_weight: bfloat16 [8, 512, 2048], P('ep', None, 'tp'), may hold values from -0.25 to 0.25
Outputs:
- mixed: bfloat16 [8192, 2048], P(('grp', 'ep'), 'tp'), parts along dimension 0
The draws below stay inside these ranges and needn't reach their ends.
There are 2 independent parts, one for each index of `grp`. The reference program is written for one: setup_inputs(seed, part) draws one part's arguments, and reference() takes and returns one part's arrays. A program takes and returns all parts, laid end to end along the dimension named above; an argument that names none is the same for every part. Nothing has to cross between parts.
Inputs may be any that keep to these rules, and one draw needn't show every extreme that they name: `expert_ids`: each token names 2 different experts. Among the 512 tokens of one index of ep (aligned blocks of rows) at most 192 name the same expert, and in some block some expert is named by exactly 192 of them.
All inputs are finite; a program needn't handle non-finite values.
Results may differ from the reference program's by a relative error of at most 0.007.
Values may be sent and summed in bfloat16 or wider, within the bound.
A program may use at most 64 MiB of HBM per device.

```python
import math
import jax
import jax.numpy as jnp
import numpy as np
from jax import lax

D = 2048
DE = 512
TOP_K = 2
TOK_DEV = 512
EXPERTS = 8
TOKENS = 4096
CAP = 192
N_EP = 8


def levels(key, dims, pieces, least, high):
    def one(dim, parts):
        draws = jax.random.uniform(jax.random.fold_in(jax.random.fold_in(key, 6), dim), (parts,), jnp.float32, least / len(pieces), high / len(pieces))
        return jnp.repeat(jnp.exp(draws), dims[dim] // parts).reshape((-1,) + (1,) * (len(dims) - dim - 1))

    factor_of = one(*pieces[0])
    for cut in pieces[1:]:
        factor_of = factor_of * one(*cut)
    return factor_of


def shared_out(own_key, own, number, rows, amount, top, bound, lean):
    sequence = jax.random.permutation(own_key, amount)
    crowded, ordinary = shares(amount, rows * top, bound, lean, True), shares(amount, rows * top, bound, lean, False)
    places = jnp.arange(amount)

    def named(lengths, turn):
        used = int((lengths > 0).sum())
        fixed = max(1, used // 4)
        passed = fixed + (places - fixed + turn * (used - fixed)) % max(1, amount - fixed)
        return jnp.zeros((amount,), jnp.int32).at[sequence[jnp.where(places < fixed, places, passed)]].set(jnp.asarray(lengths, jnp.int32))

    lengths = jnp.where(number % 4 == 0, named(crowded, number // 4), named(ordinary, number - number // 4 - 1))
    mixed = jax.random.permutation(jax.random.fold_in(own, 3), amount)
    giver, receiver = mixed[0:amount // 2 * 2:2], mixed[1:amount // 2 * 2:2]
    room = jnp.minimum(lengths[giver] - 1, bound - lengths[receiver]) // 2
    room = jnp.where((giver == sequence[0]) | (receiver == sequence[0]) | (lengths[receiver] == 0), 0, jnp.maximum(room, 0))
    passed = jax.random.randint(jax.random.fold_in(own, 4), (amount // 2,), 0, 1 << 20) % (room + 1)
    lengths = lengths.at[giver].add(-passed).at[receiver].add(passed)
    labels = jnp.searchsorted(jnp.cumsum(lengths), jnp.arange(rows * top), side="right").astype(jnp.int32)
    table = labels.reshape(top, rows).T
    table = table[jax.random.permutation(jax.random.fold_in(own, 1), rows)]
    turn = jax.random.randint(jax.random.fold_in(own, 2), (rows, 1), 0, top)
    return jnp.take_along_axis(table, (jnp.arange(top)[None, :] + turn) % top, axis=1)


def shares(amount, total, bound, lean, full):
    portions = [(1 << 20) // math.isqrt(grade ** lean) + 1 for grade in range(1, amount + 1)]
    largest = bound if full else min(bound, max(-(-total // amount), total * portions[0] // sum(portions)))
    least = 1 if total - largest >= amount - 1 else 0
    counts, surplus = [largest] + [least] * (amount - 1), total - largest - least * (amount - 1)
    while surplus > 0:
        free = [i for i in range(1, amount) if counts[i] < largest] or [i for i in range(1, amount) if counts[i] < bound]
        whole, remaining = sum([portions[i] for i in free]), surplus
        for i in free:
            extra = min(bound - counts[i], max(1, remaining * portions[i] // whole), surplus)
            counts[i] = counts[i] + extra
            surplus = surplus - extra
    return np.array(counts)


def gaussian(own_key, extent, scale, limit, split=(), kind=jnp.bfloat16):
    entries = scale * jax.random.normal(own_key, extent, jnp.float32)
    if split:
        entries = entries * levels(own_key, extent, split, -0.22, 0.18)
    return jnp.clip(entries, -limit, limit).astype(kind)


def setup_inputs(seed: int = 0, part: int = 0) -> dict:
    key_of = jax.random.split(jax.random.key(seed), 8)
    own_keys = jax.random.split(jax.random.fold_in(key_of[7], part), 8)
    tokens = gaussian(own_keys[0], (TOKENS, D), 1.0, 6.0, ((0, 8), (1, 2)))
    norm_gain = jnp.clip(1.0 + 0.18 * jax.random.normal(key_of[1], (D,), jnp.float32), 0.1, 1.9)
    expert_ids_keys = jax.random.split(jax.random.fold_in(own_keys[2], 1), TOKENS // TOK_DEV)
    expert_ids_turns = jax.random.permutation(jax.random.fold_in(own_keys[2], 3), TOKENS // TOK_DEV)
    expert_ids = jax.vmap(lambda own, number: shared_out(jax.random.fold_in(own_keys[2], 2), own, number, TOK_DEV, EXPERTS, TOP_K, CAP, 2))(expert_ids_keys, expert_ids_turns).reshape((TOKENS, TOP_K))
    route_weights = jnp.clip(jnp.exp(math.log(1.0) - 2.3025851 * jax.random.uniform(own_keys[3], (TOKENS, TOP_K), jnp.float32) ** levels(own_keys[3], (TOKENS, TOP_K), ((0, 8),), -0.2, 0.2)), 0.1, 1.0)
    gate_weight = gaussian(key_of[4], (EXPERTS, D, DE), D ** -0.5, 0.125, ((0, 8), (2, 2)))
    up_weight = gaussian(key_of[5], (EXPERTS, D, DE), D ** -0.5, 0.125, ((0, 8), (2, 2)))
    down_weight = gaussian(key_of[6], (EXPERTS, DE, D), DE ** -0.5, 0.25, ((0, 8), (2, 2)))
    return dict(tokens=tokens, norm_gain=norm_gain, expert_ids=expert_ids, route_weights=route_weights, gate_weight=gate_weight, up_weight=up_weight, down_weight=down_weight)


def reference(tokens, norm_gain, expert_ids, route_weights, gate_weight, up_weight, down_weight):
    xf = tokens.astype(jnp.float32)
    scale = lax.rsqrt(lax.optimization_barrier(jnp.mean(xf * xf, axis=-1, keepdims=True)) + 1e-06)
    normed = (xf * scale * norm_gain.astype(jnp.float32)[None, :]).astype(jnp.bfloat16)
    flat = expert_ids.reshape(-1).astype(jnp.int32)
    pairs = flat.shape[0]
    onehot = (flat[:, None] == jnp.arange(EXPERTS, dtype=jnp.int32)[None, :]).astype(jnp.int32)
    blocked = onehot.reshape(-1, TOK_DEV * TOP_K, EXPERTS)
    earlier = (jnp.cumsum(blocked, axis=1) - blocked).reshape(pairs, EXPERTS)
    slot = lax.optimization_barrier(jnp.sum(earlier * onehot, axis=-1)).astype(jnp.int32)
    block = (jnp.arange(pairs, dtype=jnp.int32) // (TOK_DEV * TOP_K)).astype(jnp.int32)
    position = (block * CAP + slot).astype(jnp.int32)
    owner = (jnp.arange(pairs, dtype=jnp.int32) // TOP_K).astype(jnp.int32)
    source = jnp.full((EXPERTS, N_EP * CAP), TOKENS, jnp.int32).at[flat, position].set(owner)
    weights = jnp.zeros((EXPERTS, N_EP * CAP), jnp.float32).at[flat, position].set(route_weights.reshape(-1).astype(jnp.float32))
    padded = jnp.concatenate([normed, jnp.zeros((1, normed.shape[1]), jnp.bfloat16)], axis=0)

    def one_expert(total, inputs):
        rows_idx, row_w, w_gate, w_up, w_down = inputs
        rows = padded[rows_idx]
        gate = jnp.dot(rows, w_gate, preferred_element_type=jnp.float32)
        upper = jnp.dot(rows, w_up, preferred_element_type=jnp.float32)
        hidden = (jax.nn.silu(gate) * upper).astype(jnp.bfloat16)
        result = jnp.dot(hidden, w_down, preferred_element_type=jnp.float32).astype(jnp.bfloat16)
        total = total.at[rows_idx].add(result.astype(jnp.float32) * row_w[:, None])
        return (total, None)
    start = jnp.zeros((TOKENS + 1, normed.shape[1]), jnp.float32)
    total, _ = lax.scan(one_expert, start, (source, weights, gate_weight, up_weight, down_weight))
    return total[:TOKENS].astype(jnp.bfloat16)
```

```python
import functools

import jax
import jax.numpy as jnp
from jax import lax
from jax.experimental import pallas as pl
from jax.experimental.pallas import tpu as pltpu
from jax.sharding import PartitionSpec as P

MESH = pl.DeviceIdType.MESH
COLS = 2
PIECES = 8
LEAD = 2
CUTS = 4


def normalize(rows, norm_gain):
    xf = rows.astype(jnp.float32)
    scale = lax.rsqrt(jnp.mean(xf * xf, axis=-1, keepdims=True) + 1e-06)
    return (xf * scale * norm_gain[None, :]).astype(jnp.bfloat16)


def sparse_form(tokens, norm_gain, expert_ids, route_weights, gate_weight, up_weight, down_weight):
    tok_rows, half = tokens.shape
    width = half * lax.axis_size("tp")
    experts = lax.axis_size("ep")
    top = expert_ids.shape[1]
    capacity = max(2, (3 * tok_rows * top + 2 * experts - 1) // (2 * experts))
    flat = expert_ids.reshape(-1)
    onehot = (flat[:, None] == jnp.arange(experts, dtype=jnp.int32)[None, :]).astype(jnp.int32)
    earlier = jnp.cumsum(onehot, axis=0) - onehot
    slot = jnp.sum(earlier * onehot, axis=-1)
    position = flat * capacity + slot
    owner = jnp.arange(flat.shape[0], dtype=jnp.int32) // top
    w_gate = gate_weight[0]
    w_up = up_weight[0]
    w_down = down_weight[0]
    send = jnp.zeros((experts * capacity, half), jnp.bfloat16).at[position].set(tokens[owner])
    send = send.reshape(experts, capacity, half)
    received = lax.all_to_all(send, "ep", split_axis=0, concat_axis=0, tiled=True)
    sources = received.shape[0]
    count = received.shape[1]
    whole_rows = lax.all_gather(received, "tp", axis=2, tiled=True)
    rows = normalize(whole_rows.reshape(sources * count, width), norm_gain)
    gate = jnp.dot(rows, w_gate, preferred_element_type=jnp.float32)
    upper = jnp.dot(rows, w_up, preferred_element_type=jnp.float32)
    hidden = (jax.nn.silu(gate) * upper).astype(jnp.bfloat16)
    result = jnp.dot(
        lax.all_gather(hidden, "tp", axis=1, tiled=True), w_down, preferred_element_type=jnp.float32
    )
    result = result.astype(jnp.bfloat16).reshape(sources, count, half)
    back = lax.all_to_all(result, "ep", split_axis=0, concat_axis=0, tiled=True)
    picked = back.reshape(experts * capacity, half)[position].astype(jnp.float32)
    picked = picked * route_weights.reshape(-1)[:, None]
    return jnp.sum(picked.reshape(tok_rows, top, half), axis=1).astype(jnp.bfloat16)


def line_kernel(
    length, cap, tok_ref, gain_ref, route_ref, gate_in, up_in, down_in, out_ref,
    raw, x, wt, wg, wu, wd, hid, part, came, slim, slim_in, acc,
    swap_s, swap_r, loc, wy_s, wy_r, wx_s, wx_r, gat_s, gat_r, tab_s, tab_r,
    half_s, half_r, hid_s, hid_r, sum_s, sum_r, slim_s, slim_r,
):
    f32, bf16 = jnp.float32, jnp.bfloat16
    g, ep, c = lax.axis_index("grp"), lax.axis_index("ep"), lax.axis_index("tp")
    z, y = ep // COLS, ep % COLS
    last = length - 1
    flip = z >= length // 2
    end = jnp.where(flip, last, 0)
    mid = jnp.where(flip, last - 1, 1)
    far_mid, far_end = last - mid, last - end
    outer, inner = z == end, z == mid
    mate, across, beside = {"tp": 1 - c}, {"grp": 1 - g}, {"ep": z * COLS + 1 - y}
    to_end, to_mid, to_far = {"ep": end * COLS + y}, {"ep": mid * COLS + y}, {"ep": far_mid * COLS + y}
    rows, half = raw.shape
    piece = rows // PIECES
    unit = rows // 2
    per_unit = PIECES // 2
    wide = hid.shape[3]

    def remote(src, dst, ss, rs, dev):
        return pltpu.make_async_remote_copy(
            src_ref=src, dst_ref=dst, send_sem=ss, recv_sem=rs, device_id=dev, device_id_type=MESH
        )

    def span(q):
        return pl.ds(q * piece if isinstance(q, int) else pl.multiple_of(q * piece, piece), piece)

    barrier = pltpu.get_barrier_semaphore()
    for dev in (mate, across, beside):
        pl.semaphore_signal(barrier, inc=1, device_id=dev, device_id_type=MESH)

    @pl.when(outer)
    def _():
        pl.semaphore_signal(barrier, inc=1, device_id=to_mid, device_id_type=MESH)

    @pl.when(inner)
    def _():
        pl.semaphore_signal(barrier, inc=1, device_id=to_end, device_id_type=MESH)
        pl.semaphore_signal(barrier, inc=1, device_id=to_far, device_id_type=MESH)

    pl.semaphore_wait(barrier, jnp.where(outer, 4, 5))

    def swap(q):
        return remote(tok_ref.at[span(q)], raw.at[span(q)], swap_s.at[q], swap_r.at[q], mate)

    for q in range(PIECES):
        swap(q).start()

    mats = ((gate_in, wg), (up_in, wu), (down_in, wd))
    chunks = []
    for m in range(3):
        size = mats[m][0].shape[0] // (2 * CUTS)
        for u in range(CUTS):
            chunks.append((m, u, size))
    amount = len(chunks)

    def cut(portion, u, size):
        return pl.ds(pl.multiple_of((portion * CUTS + u) * size, size), size)

    def send_y(t):
        m, u, q = chunks[t]
        src, dst = mats[m]
        return remote(src.at[cut(g, u, q)], dst.at[1, cut(g, u, q)], wy_s.at[t], wy_r.at[t], beside)

    def send_x(t, portion):
        m, u, q = chunks[t]
        buf = mats[m][1].at[1, cut(portion, u, q)]
        return remote(buf, buf, wx_s.at[t], wx_r.at[t], across)

    for t in range(amount):
        send_y(t).start()
    local = [pltpu.make_async_copy(mats[m][0], mats[m][1].at[0], loc.at[m]) for m in range(3)]
    for copy in local:
        copy.start()

    def gather(b, q, way, dev):
        at = x.at[b, c, span(q)]
        return remote(at, at, gat_s.at[way, b, q], gat_r.at[b, q], dev)

    def table(b, way, dev, src=None):
        src = wt.at[b] if src is None else src
        return remote(src, wt.at[b], tab_s.at[way, b], tab_r.at[b], dev)

    def share(b, q, side):
        at = x.at[b, side, span(q)]
        return remote(at, at, half_s.at[b, q], half_r.at[b, q], mate)

    def total(b, q, dev):
        return remote(part.at[b, span(q)], came.at[b, span(q)], sum_s.at[b, q], sum_r.at[b, q], dev)

    def compact(s, dev):
        return remote(slim.at[s], slim_in.at[s], slim_s.at[s], slim_r.at[s], dev)

    def hand(slot, side, count):
        at = hid.at[slot, side, pl.ds(0, count)]
        return remote(at, at, hid_s.at[slot], hid_r.at[slot], mate)

    @pl.when(outer)
    def _():
        table(z, 0, to_mid, route_ref).start()

    @pl.when(inner)
    def _():
        table(z, 0, to_end, route_ref).start()
        table(z, 1, to_far, route_ref).start()

    wt[z] = route_ref[...]

    def norm(q, carry):
        swap(q).wait_recv()
        at = span(q)
        a = tok_ref[at].astype(f32)
        b = raw[at].astype(f32)
        total_sq = jnp.sum(a * a, axis=-1, keepdims=True) + jnp.sum(b * b, axis=-1, keepdims=True)
        scale = lax.rsqrt(total_sq / (2 * half) + 1e-06)
        x[z, c, at] = (a * scale * gain_ref[c]).astype(bf16)
        x[z, 1 - c, at] = (b * scale * gain_ref[1 - c]).astype(bf16)

        @pl.when(outer)
        def _():
            gather(z, q, 0, to_mid).start()

        @pl.when(inner)
        def _():
            gather(z, q, 0, to_end).start()

            @pl.when(q < LEAD)
            def _():
                gather(z, q, 1, to_far).start()
        return carry

    lax.fori_loop(0, PIECES, norm, 0)

    def got_y(t):
        send_y(t).wait_recv()
        send_x(t, g).start()

    def outer_stream(j):
        b = (mid, far_end, far_mid)[j // PIECES]
        q = j % PIECES
        gather(b, q, 0, to_mid).wait_recv()
        share(b, q, c).start()

    def inner_stream(j):
        if j < LEAD:
            b, q = far_mid, j
        elif j < LEAD + PIECES:
            b, q = far_end, j - LEAD
        else:
            b, q = far_mid, j - PIECES
        gather(b, q, 1, to_far).wait_recv()
        share(b, q, c).start()
        if j >= LEAD:
            gather(b, q, 0, to_end).start()
        if j == LEAD + PIECES - 1:
            for early in range(LEAD):
                gather(far_mid, early, 0, to_end).start()

    def inner_end(q):
        gather(end, q, 0, to_end).wait_recv()
        share(end, q, c).start()
        gather(end, q, 1, to_far).start()
        if q == PIECES - 1:
            for late in range(LEAD, PIECES):
                gather(z, late, 1, to_far).start()

    def pick(table_rows, e):
        lane = lax.broadcasted_iota(jnp.int32, table_rows.shape, 0)
        return jnp.sum(jnp.where(lane == e, table_rows, 0.0), axis=0, keepdims=True)

    def selection(b, e):
        weights = wt[b]
        chosen = jnp.where(weights > 0.0, 1.0, 0.0)
        above = lax.broadcasted_iota(jnp.int32, (rows, rows), 0)
        along = lax.broadcasted_iota(jnp.int32, (rows, rows), 1)
        before = jnp.where(above < along, 1.0, 0.0).astype(bf16)
        rank = jnp.dot(chosen.astype(bf16), before, preferred_element_type=f32)
        place = pick(jnp.where(chosen > 0.0, rank, -1.0), e)
        slot = lax.broadcasted_iota(jnp.int32, (cap, rows), 0).astype(f32)
        return jnp.where(slot == place, 1.0, 0.0), pick(weights, e)

    def hidden_half(first, second, s):
        both = []
        for w in (wg, wu):
            both.append(
                jnp.dot(first, w[s, :half], preferred_element_type=f32)
                + jnp.dot(second, w[s, half:], preferred_element_type=f32)
            )
        gate, upper = both
        return (gate * (0.5 * (1.0 + jnp.tanh(0.5 * gate))) * upper).astype(bf16)

    def lowered(slot, s, count):
        at = pl.ds(0, count)
        return jnp.dot(hid[slot, 0, at], wd[s, :wide], preferred_element_type=f32) + jnp.dot(
            hid[slot, 1, at], wd[s, wide:], preferred_element_type=f32
        )

    def slim_rows(s):
        slot = 4 * length + s
        mark, weight_row = selection(mid, end * COLS + (y if s == 0 else 1 - y))
        ones = mark.astype(bf16)
        first = jnp.dot(ones, x[mid, 0], preferred_element_type=f32).astype(bf16)
        second = jnp.dot(ones, x[mid, 1], preferred_element_type=f32).astype(bf16)
        hid[slot, c, pl.ds(0, cap)] = hidden_half(first, second, s)
        hand(slot, c, cap).start()
        weight = jnp.sum(mark * weight_row, axis=1, keepdims=True)
        hand(slot, 1 - c, cap).wait_recv()
        slim[s] = (lowered(slot, s, cap) * weight).astype(bf16)
        compact(s, to_mid).start()

    def widen(s, at):
        mark, _ = selection(mid, end * COLS + (y if s == 0 else 1 - y))
        ones = mark.astype(bf16)
        return lax.dot_general(ones, slim_in[s], (((0,), (0,)), ((), ())), preferred_element_type=f32)

    def dense_unit(b, part_of, slot):
        at = pl.ds(pl.multiple_of(part_of * unit, unit), unit)
        columns = wt[b, :, at].T
        lane = lax.broadcasted_iota(jnp.int32, columns.shape, 1)
        first, second = x[b, 0, at], x[b, 1, at]
        for s in range(2):
            hid[slot + s, c] = hidden_half(first, second, s)
            hand(slot + s, c, unit).start()
        sums = None
        for s in range(2):
            expert = z * COLS + (y if s == 0 else 1 - y)
            weight = jnp.sum(jnp.where(lane == expert, columns, 0.0), axis=1, keepdims=True)
            hand(slot + s, 1 - c, unit).wait_recv()
            got = lowered(slot + s, s, unit) * weight
            sums = got if sums is None else sums + got

        @pl.when(b == z)
        def _():
            acc[at] = sums

        @pl.when(b != z)
        def _():
            part[b, at] = sums.astype(bf16)

    def pass_on(b, q, dev):
        total(b, q, dev).wait_recv()
        at = span(q)
        part[b, at] = (part[b, at].astype(f32) + came[b, at].astype(f32)).astype(bf16)
        total(b, q, dev).start()

    def take_in(q):
        total(z, q, to_far).wait_recv()
        at = span(q)
        acc[at] = acc[at] + came[z, at].astype(f32)

    @pl.when(outer)
    def _():
        table(mid, 0, to_mid).wait_recv()
        for j in range(amount):
            outer_stream(j)
            got_y(j)
            if j == PIECES + 1:
                for q in range(PIECES):
                    share(mid, q, 1 - c).wait_recv()
                for m in range(3):
                    local[m].wait()
                slim_rows(0)
        table(far_end, 0, to_mid).wait_recv()
        table(far_mid, 0, to_mid).wait_recv()

    @pl.when(inner)
    def _():
        table(end, 0, to_end).wait_recv()
        table(end, 1, to_far).start()
        table(far_mid, 1, to_far).wait_recv()
        table(far_mid, 0, to_end).start()
        for j in range(amount):
            if j < PIECES:
                inner_end(j)
            inner_stream(j)
            got_y(j)
            if j == PIECES:
                table(far_end, 1, to_far).wait_recv()
                table(far_end, 0, to_end).start()
        for m in range(3):
            local[m].wait()

    for t in range(amount):
        send_x(t, 1 - g).wait_recv()

    def step(i, carry):
        k, part_of = i // 2, i % 2
        b = jnp.where(k == 0, far_end, jnp.where(k == 1, end, jnp.where(k == 2, far_mid, mid)))

        @pl.when(outer)
        def _():
            for n in range(2):
                @pl.when(i == n)
                def _():
                    for q in range(n * per_unit, (n + 1) * per_unit):
                        if PIECES + q >= amount:
                            outer_stream(PIECES + q)
                    for q in range(n * per_unit, (n + 1) * per_unit):
                        share(far_end, q, 1 - c).wait_recv()

                @pl.when(i == 4 + n)
                def _():
                    for q in range(n * per_unit, (n + 1) * per_unit):
                        outer_stream(2 * PIECES + q)
                    for q in range(n * per_unit, (n + 1) * per_unit):
                        share(far_mid, q, 1 - c).wait_recv()

            @pl.when(i == 6)
            def _():
                slim_rows(1)

        @pl.when(inner)
        def _():
            rest = 2 * PIECES - amount
            for n in range(2):
                @pl.when(i == n)
                def _():
                    for q in range(n * per_unit, (n + 1) * per_unit):
                        share(far_end, q, 1 - c).wait_recv()

                @pl.when(i == 2 + n)
                def _():
                    for j in range(amount + n * rest // 2, amount + (n + 1) * rest // 2):
                        inner_stream(j)
                    for q in range(n * per_unit, (n + 1) * per_unit):
                        share(end, q, 1 - c).wait_recv()

                @pl.when(i == 4 + n)
                def _():
                    for q in range(n * per_unit, (n + 1) * per_unit):
                        share(far_mid, q, 1 - c).wait_recv()
            for n in range(4):
                @pl.when(i == 4 + n)
                def _():
                    for q in range(n * PIECES // 4, (n + 1) * PIECES // 4):
                        pass_on(far_end, q, to_far)
                    if n >= 2:
                        for q in range((n - 2) * PIECES // 4, (n - 1) * PIECES // 4):
                            pass_on(end, q, to_end)

        @pl.when(inner | (k < 3))
        def _():
            dense_unit(b, part_of, 2 * i)

        @pl.when(outer & ((k == 0) | (k == 2)))
        def _():
            for n in range(per_unit):
                total(b, part_of * per_unit + n, to_mid).start()
        return carry

    lax.fori_loop(0, 2 * length, step, 0)

    @pl.when(outer)
    def _():
        for q in range(PIECES):
            total(z, q, to_mid).wait_recv()
            at = span(q)
            out_ref[at] = (acc[at] + came[z, at].astype(f32)).astype(bf16)

    @pl.when(inner)
    def _():
        compact(0, to_end).wait_recv()
        acc[...] = acc[...] + widen(0, None)
        for q in range(PIECES // 2, PIECES):
            pass_on(end, q, to_end)
        for q in range(PIECES):
            pass_on(far_mid, q, to_far)
            if q >= 2:
                take_in(q - 2)
        for q in range(PIECES - 2, PIECES):
            take_in(q)
        compact(1, to_end).wait_recv()
        out_ref[...] = (acc[...] + widen(1, None)).astype(bf16)

    for q in range(PIECES):
        swap(q).wait_send()
    for t in range(amount):
        send_y(t).wait_send()
        send_x(t, g).wait_send()

    @pl.when(outer)
    def _():
        table(z, 0, to_mid, route_ref).wait_send()
        for s in range(2):
            compact(s, to_mid).wait_send()
            hand(4 * length + s, c, cap).wait_send()
        for slot in range(4 * length - 4):
            hand(slot, c, unit).wait_send()
        for q in range(PIECES):
            gather(z, q, 0, to_mid).wait_send()
            for b in (far_end, far_mid):
                total(b, q, to_mid).wait_send()
            for b in (mid, far_end, far_mid):
                share(b, q, c).wait_send()

    @pl.when(inner)
    def _():
        for slot in range(4 * length):
            hand(slot, c, unit).wait_send()
        table(z, 0, to_end, route_ref).wait_send()
        table(z, 1, to_far, route_ref).wait_send()
        table(end, 1, to_far).wait_send()
        table(far_mid, 0, to_end).wait_send()
        table(far_end, 0, to_end).wait_send()
        for q in range(PIECES):
            for b in (z, far_mid, far_end):
                gather(b, q, 0, to_end).wait_send()
            for b in (z, end):
                gather(b, q, 1, to_far).wait_send()
            total(end, q, to_end).wait_send()
            for b in (far_mid, far_end):
                total(b, q, to_far).wait_send()
            for b in (end, far_mid, far_end):
                share(b, q, c).wait_send()


def line_form(tokens, norm_gain, expert_ids, route_weights, gate_weight, up_weight, down_weight):
    tok_rows, half = tokens.shape
    experts = lax.axis_size("ep")
    length = experts // COLS
    top = expert_ids.shape[1]
    cap = (3 * tok_rows * top + 2 * experts - 1) // (2 * experts)
    bf16, f32 = jnp.bfloat16, jnp.float32
    chosen = expert_ids[None] == jnp.arange(experts, dtype=jnp.int32)[:, None, None]
    route = jnp.sum(jnp.where(chosen, route_weights[None], 0.0), axis=-1)
    gate, up, down = gate_weight[0], up_weight[0], down_weight[0]
    dma, vmem = pltpu.SemaphoreType.DMA, pltpu.VMEM
    block = (length, tok_rows, half)
    slots = 4 * length + 2
    cuts, bits = (3 * CUTS,), (length, PIECES)
    sems = [dma((PIECES,)), dma((PIECES,)), dma((3,))]
    for send, recv in (
        (cuts, cuts), (cuts, cuts), ((2,) + bits, bits), ((2, length), (length,)),
        (bits, bits), ((slots,), (slots,)), (bits, bits), ((2,), (2,)),
    ):
        sems += [dma(send), dma(recv)]
    return pl.pallas_call(
        functools.partial(line_kernel, length, cap),
        out_shape=jax.ShapeDtypeStruct((tok_rows, half), bf16),
        in_specs=[pl.BlockSpec(memory_space=vmem)] * 3 + [pl.BlockSpec(memory_space=pl.ANY)] * 3,
        out_specs=pl.BlockSpec(memory_space=vmem),
        scratch_shapes=[
            vmem((tok_rows, half), bf16),
            vmem((length, 2, tok_rows, half), bf16),
            vmem((length, experts, tok_rows), f32),
            vmem((2,) + gate.shape, bf16),
            vmem((2,) + up.shape, bf16),
            vmem((2,) + down.shape, bf16),
            vmem((slots, 2, tok_rows // 2, gate.shape[1]), bf16),
            vmem(block, bf16),
            vmem(block, bf16),
            vmem((2, cap, half), bf16),
            vmem((2, cap, half), bf16),
            vmem((tok_rows, half), f32),
        ]
        + sems,
        compiler_params=pltpu.CompilerParams(
            collective_id=0, has_side_effects=True, vmem_limit_bytes=60 * 1024 * 1024
        ),
    )(tokens, norm_gain.reshape(2, 1, half), route, gate, up, down)


def solution(mesh):
    in_specs = (
        P(("grp", "ep"), "tp"),
        P(),
        P(("grp", "ep"), None),
        P(("grp", "ep"), None),
        P("ep", None, "tp"),
        P("ep", None, "tp"),
        P("ep", None, "tp"),
    )
    out_specs = P(("grp", "ep"), "tp")
    shape = mesh.shape

    def on_device(tokens, norm_gain, expert_ids, *rest):
        dense = shape["ep"] == 4 * COLS and shape["ep"] == 4 * expert_ids.shape[1]
        form = line_form if dense and shape["grp"] == 2 and shape["tp"] == 2 else sparse_form
        return form(tokens, norm_gain, expert_ids, *rest)

    return jax.shard_map(
        on_device, mesh=mesh, in_specs=in_specs, out_specs=out_specs, check_vma=False
    )
```

```python
import functools

import jax
import jax.numpy as jnp
from jax import lax
from jax.experimental import pallas as pl
from jax.experimental.pallas import tpu as pltpu
from jax.sharding import PartitionSpec as P

MESH = pl.DeviceIdType.MESH
COLS = 2
PIECES = 8
UNITS = 4
LEAD = 2
CUTS = 8


def normalize(rows, norm_gain):
    xf = rows.astype(jnp.float32)
    scale = lax.rsqrt(jnp.mean(xf * xf, axis=-1, keepdims=True) + 1e-06)
    return (xf * scale * norm_gain[None, :]).astype(jnp.bfloat16)


def sparse_form(tokens, norm_gain, expert_ids, route_weights, gate_weight, up_weight, down_weight):
    tok_rows, half = tokens.shape
    width = half * lax.axis_size("tp")
    experts = lax.axis_size("ep")
    top = expert_ids.shape[1]
    capacity = max(2, (3 * tok_rows * top + 2 * experts - 1) // (2 * experts))
    flat = expert_ids.reshape(-1)
    onehot = (flat[:, None] == jnp.arange(experts, dtype=jnp.int32)[None, :]).astype(jnp.int32)
    earlier = jnp.cumsum(onehot, axis=0) - onehot
    slot = jnp.sum(earlier * onehot, axis=-1)
    position = flat * capacity + slot
    owner = jnp.arange(flat.shape[0], dtype=jnp.int32) // top
    w_gate = gate_weight[0]
    w_up = up_weight[0]
    w_down = down_weight[0]
    send = jnp.zeros((experts * capacity, half), jnp.bfloat16).at[position].set(tokens[owner])
    send = send.reshape(experts, capacity, half)
    received = lax.all_to_all(send, "ep", split_axis=0, concat_axis=0, tiled=True)
    sources = received.shape[0]
    count = received.shape[1]
    whole_rows = lax.all_gather(received, "tp", axis=2, tiled=True)
    rows = normalize(whole_rows.reshape(sources * count, width), norm_gain)
    gate = jnp.dot(rows, w_gate, preferred_element_type=jnp.float32)
    upper = jnp.dot(rows, w_up, preferred_element_type=jnp.float32)
    hidden = (jax.nn.silu(gate) * upper).astype(jnp.bfloat16)
    result = jnp.dot(
        lax.all_gather(hidden, "tp", axis=1, tiled=True), w_down, preferred_element_type=jnp.float32
    )
    result = result.astype(jnp.bfloat16).reshape(sources, count, half)
    back = lax.all_to_all(result, "ep", split_axis=0, concat_axis=0, tiled=True)
    picked = back.reshape(experts * capacity, half)[position].astype(jnp.float32)
    picked = picked * route_weights.reshape(-1)[:, None]
    return jnp.sum(picked.reshape(tok_rows, top, half), axis=1).astype(jnp.bfloat16)


def line_kernel(
    length, cap, tok_ref, gain_in, ids_in, route_in, gate_in, up_in, down_in, out_ref,
    own, gain_ref, ids_ref, route_ref, raw, x, wt, columns, wg, wu, wd, hid, slim_hid, part, came, slim, slim_in, acc,
    swap_s, swap_r, loc, wy_s, wy_r, wx_s, wx_r, gat_s, gat_r, tab_s, tab_r,
    half_s, half_r, hid_s, hid_r, few_s, few_r, sum_s, sum_r, slim_s, slim_r,
):
    f32, bf16 = jnp.float32, jnp.bfloat16
    g, ep, c = lax.axis_index("grp"), lax.axis_index("ep"), lax.axis_index("tp")
    z, y = ep // COLS, ep % COLS
    last = length - 1
    flip = z >= length // 2
    end = jnp.where(flip, last, 0)
    mid = jnp.where(flip, last - 1, 1)
    far_mid, far_end = last - mid, last - end
    outer, inner = z == end, z == mid
    mate, across, beside = {"tp": 1 - c}, {"grp": 1 - g}, {"ep": z * COLS + 1 - y}
    to_end, to_mid, to_far = {"ep": end * COLS + y}, {"ep": mid * COLS + y}, {"ep": far_mid * COLS + y}
    rows, half = raw.shape
    piece = rows // PIECES
    unit = rows // UNITS
    per_unit = PIECES // UNITS
    wide = hid.shape[3]

    def remote(src, dst, ss, rs, dev):
        return pltpu.make_async_remote_copy(
            src_ref=src, dst_ref=dst, send_sem=ss, recv_sem=rs, device_id=dev, device_id_type=MESH
        )

    def span(q):
        return pl.ds(q * piece if isinstance(q, int) else pl.multiple_of(q * piece, piece), piece)

    barrier = pltpu.get_barrier_semaphore()
    for dev in (mate, across, beside):
        pl.semaphore_signal(barrier, inc=1, device_id=dev, device_id_type=MESH)

    @pl.when(outer)
    def _():
        pl.semaphore_signal(barrier, inc=1, device_id=to_mid, device_id_type=MESH)

    @pl.when(inner)
    def _():
        pl.semaphore_signal(barrier, inc=1, device_id=to_end, device_id_type=MESH)
        pl.semaphore_signal(barrier, inc=1, device_id=to_far, device_id_type=MESH)

    inputs = ((tok_ref, own), (gain_in, gain_ref), (ids_in, ids_ref), (route_in, route_ref))
    inputs += ((gate_in, wg.at[0]), (up_in, wu.at[0]), (down_in, wd.at[0]))
    local = [pltpu.make_async_copy(src, dst, loc.at[k]) for k, (src, dst) in enumerate(inputs)]
    for copy in local:
        copy.start()
    pl.semaphore_wait(barrier, jnp.where(outer, 4, 5))

    mats = ((gate_in, wg), (up_in, wu), (down_in, wd))

    def cut(m, portion, u, many=1):
        size = mats[m][0].shape[0] // (2 * CUTS)
        return pl.ds(pl.multiple_of((portion * CUTS + u) * size, size), size * many)

    def send_y(m, u, many=1):
        src, dst = mats[m]
        at = cut(m, g, u, many)
        return remote(src.at[at], dst.at[1, at], wy_s.at[m], wy_r.at[m, u], beside)

    def send_x(m, u, portion, many=1):
        buf = mats[m][1].at[1, cut(m, portion, u, many)]
        return remote(buf, buf, wx_s.at[m], wx_r.at[m], across)

    for m in range(3):
        for u in range(CUTS):
            send_y(m, u).start()

    def swap(q, many=1):
        at = pl.ds(q * piece if isinstance(q, int) else pl.multiple_of(q * piece, piece), piece * many)
        return remote(own.at[at], raw.at[at], swap_s, swap_r.at[q], mate)

    local[0].wait()
    for q in range(PIECES):
        swap(q).start()
    for copy in local[1:4]:
        copy.wait()

    def gather(b, q, way, dev):
        at = x.at[b, c, span(q)]
        return remote(at, at, gat_s.at[way, b], gat_r.at[b, q], dev)

    def gather_sent(b, way, dev):
        remote(x.at[b, c], x.at[b, c], gat_s.at[way, b], gat_r.at[b, 0], dev).wait_send()

    def table(b, way, dev):
        return remote(wt.at[b], wt.at[b], tab_s.at[way, b], tab_r.at[b], dev)

    def share(b, q):
        at = x.at[b, c, span(q)]
        return remote(at, at, half_s.at[b], half_r.at[b, q // per_unit], mate)

    def shared(b, part_of):
        at = x.at[b, 1 - c, rows_of(part_of)]
        remote(at, at, half_s.at[b], half_r.at[b, part_of], mate).wait_recv()

    def rows_of(part_of):
        return pl.ds(part_of * unit if isinstance(part_of, int) else pl.multiple_of(part_of * unit, unit), unit)

    def total(b, q, dev):
        return remote(part.at[b, span(q)], came.at[b, span(q)], sum_s.at[b], sum_r.at[b, q], dev)

    def total_sent(b, dev):
        remote(part.at[b], came.at[b], sum_s.at[b], sum_r.at[b, 0], dev).wait_send()

    def compact(s, dev):
        return remote(slim.at[s], slim_in.at[s], slim_s, slim_r.at[s], dev)

    def hand(pair, s):
        at = hid.at[2 * pair + s, c]
        return remote(at, at, hid_s, hid_r.at[pair], mate)

    def hand_few(s, side):
        at = slim_hid.at[s, side]
        return remote(at, at, few_s, few_r.at[s], mate)

    named = lax.broadcasted_iota(jnp.int32, wt.shape[1:], 0)
    routes = None
    for k in range(ids_ref.shape[0]):
        term = jnp.where(named == ids_ref[pl.ds(k, 1)], route_ref[pl.ds(k, 1)], 0.0)
        routes = term if routes is None else routes + term
    wt[z] = routes

    @pl.when(outer)
    def _():
        table(z, 0, to_mid).start()

    @pl.when(inner)
    def _():
        table(z, 0, to_end).start()
        table(z, 1, to_far).start()

    def norm(q, carry):
        swap(q).wait_recv()
        at = span(q)
        a = own[at].astype(f32)
        b = raw[at].astype(f32)
        total_sq = jnp.sum(a * a, axis=-1, keepdims=True) + jnp.sum(b * b, axis=-1, keepdims=True)
        scale = lax.rsqrt(total_sq / (2 * half) + 1e-06)
        x[z, c, at] = (a * scale * gain_ref[c]).astype(bf16)
        x[z, 1 - c, at] = (b * scale * gain_ref[1 - c]).astype(bf16)

        @pl.when(outer)
        def _():
            gather(z, q, 0, to_mid).start()

        @pl.when(inner)
        def _():
            gather(z, q, 0, to_end).start()

            @pl.when(q < LEAD)
            def _():
                gather(z, q, 1, to_far).start()
        return carry

    lax.fori_loop(0, PIECES, norm, 0)
    columns[z] = wt[z].T

    def got_y(n):
        for m in range(3):
            @pl.when(n // (CUTS // 2) == m)
            def _():
                for v in range(2):
                    u = n % (CUTS // 2) * 2 + v
                    send_y(m, u).wait_recv()
                    send_x(m, u, g).start()

    def got_x(m):
        send_x(m, 0, 1 - g, CUTS).wait_recv()

    def outer_stream(j):
        b = jnp.where(j < PIECES, mid, jnp.where(j < 2 * PIECES, far_end, far_mid))
        q = j % PIECES
        gather(b, q, 0, to_mid).wait_recv()
        share(b, q).start()

    def inner_stream(j):
        lead = j < LEAD
        turn = (j >= LEAD) & (j < LEAD + PIECES)
        b = jnp.where(turn, far_end, far_mid)
        q = jnp.where(lead, j, jnp.where(turn, j - LEAD, j - PIECES))
        gather(b, q, 1, to_far).wait_recv()
        share(b, q).start()

        @pl.when(j >= LEAD)
        def _():
            gather(b, q, 0, to_end).start()

        @pl.when(j == LEAD + PIECES - 1)
        def _():
            for early in range(LEAD):
                gather(far_mid, early, 0, to_end).start()

    def inner_end(q):
        gather(end, q, 0, to_end).wait_recv()
        share(end, q).start()
        gather(end, q, 1, to_far).start()

        @pl.when(q == PIECES - 1)
        def _():
            for late in range(LEAD, PIECES):
                gather(z, late, 1, to_far).start()

    def pick(table_rows, e):
        lane = lax.broadcasted_iota(jnp.int32, table_rows.shape, 0)
        return jnp.sum(jnp.where(lane == e, table_rows, 0.0), axis=0, keepdims=True)

    def selection(b, e):
        weights = wt[b]
        chosen = jnp.where(weights > 0.0, 1.0, 0.0)
        above = lax.broadcasted_iota(jnp.int32, (rows, rows), 0)
        along = lax.broadcasted_iota(jnp.int32, (rows, rows), 1)
        before = jnp.where(above < along, 1.0, 0.0).astype(bf16)
        rank = jnp.dot(chosen.astype(bf16), before, preferred_element_type=f32)
        place = pick(jnp.where(chosen > 0.0, rank, -1.0), e)
        slot = lax.broadcasted_iota(jnp.int32, (cap, rows), 0).astype(f32)
        return jnp.where(slot == place, 1.0, 0.0), pick(weights, e)

    def hidden_half(first, second, s):
        both = []
        for w in (wg, wu):
            both.append(
                jnp.dot(first, w[s, :half], preferred_element_type=f32)
                + jnp.dot(second, w[s, half:], preferred_element_type=f32)
            )
        gate, upper = both
        return (gate * (0.5 * (1.0 + jnp.tanh(0.5 * gate))) * upper).astype(bf16)

    def lowered(left, right, s):
        return jnp.dot(left, wd[s, :wide], preferred_element_type=f32) + jnp.dot(
            right, wd[s, wide:], preferred_element_type=f32
        )

    def slim_rows(s):
        mark, weight_row = selection(mid, end * COLS + (y if s == 0 else 1 - y))
        ones = mark.astype(bf16)
        first = jnp.dot(ones, x[mid, 0], preferred_element_type=f32).astype(bf16)
        second = jnp.dot(ones, x[mid, 1], preferred_element_type=f32).astype(bf16)
        slim_hid[s, c] = hidden_half(first, second, s)
        hand_few(s, c).start()
        weight = jnp.sum(mark * weight_row, axis=1, keepdims=True)
        hand_few(s, 1 - c).wait_recv()
        slim[s] = (lowered(slim_hid[s, 0], slim_hid[s, 1], s) * weight).astype(bf16)

    def widen(s):
        mark, _ = selection(mid, end * COLS + (y if s == 0 else 1 - y))
        ones = mark.astype(bf16)
        return lax.dot_general(ones, slim_in[s], (((0,), (0,)), ((), ())), preferred_element_type=f32)

    def block_of(k):
        return jnp.where(k == 0, far_end, jnp.where(k == 1, end, jnp.where(k == 2, far_mid, mid)))

    def first_stage(code):
        pair, s = code // 2, code % 2
        b, part_of = block_of(pair // UNITS), pair % UNITS

        @pl.when((s == 0) & (b != z))
        def _():
            shared(b, part_of)

        at = rows_of(part_of)
        hid[code, c] = hidden_half(x[b, 0, at], x[b, 1, at], s)
        hand(pair, s).start()

    def second_stage(pair):
        b, part_of = block_of(pair // UNITS), pair % UNITS
        at = rows_of(part_of)
        mine = columns[b, at]
        lane = lax.broadcasted_iota(jnp.int32, mine.shape, 1)
        both = hid.at[pl.ds(2 * pair, 2), 1 - c]
        remote(both, both, hid_s, hid_r.at[pair], mate).wait_recv()
        sums = None
        for s in range(2):
            expert = z * COLS + (y if s == 0 else 1 - y)
            weight = jnp.sum(jnp.where(lane == expert, mine, 0.0), axis=1, keepdims=True)
            got = lowered(hid[2 * pair + s, 0], hid[2 * pair + s, 1], s) * weight
            sums = got if sums is None else sums + got

        @pl.when(b == z)
        def _():
            acc[at] = sums

        @pl.when(b != z)
        def _():
            part[b, at] = sums.astype(bf16)

        @pl.when(outer & (b != z))
        def _():
            for n in range(per_unit):
                total(b, part_of * per_unit + n, to_mid).start()

    def pass_on(b, q, dev):
        total(b, q, dev).wait_recv()
        at = span(q)
        part[b, at] = (part[b, at].astype(f32) + came[b, at].astype(f32)).astype(bf16)
        total(b, q, dev).start()

    def take_in(q):
        total(z, q, to_far).wait_recv()
        at = span(q)
        acc[at] = acc[at] + came[z, at].astype(f32)

    def look(n, entries):
        value = 0
        for at, entry in entries.items():
            value = jnp.where(n == at, entry, value)
        return value

    head = 3 * CUTS // 2
    outer_first = {
        0: ((1, 0, 0), (1, 1, 0)), 1: ((1, 2, 0), (1, 3, 0)), 11: ((0, 0, 0), (0, 0, 1)), 12: ((0, 1, 0), (0, 1, 1)),
        13: ((1, 0, 1), (1, 1, 1)), 14: ((0, 2, 0), (0, 2, 1)), 15: ((1, 2, 1), (1, 3, 1)), 17: ((0, 3, 0), (0, 3, 1)),
        19: ((2, 0, 0), (2, 0, 1)), 21: ((2, 1, 0), (2, 1, 1)), 23: ((2, 2, 0), (2, 2, 1)), 25: ((2, 3, 0), (2, 3, 1)),
    }
    outer_second = {
        11: ((0, 0),), 12: ((0, 1),), 14: ((0, 2),), 16: ((1, 0), (1, 1)), 17: ((0, 3),), 18: ((1, 2), (1, 3)),
        19: ((2, 0),), 21: ((2, 1),), 23: ((2, 2),), 25: ((2, 3),),
    }
    outer_pairs = {13: 13, 16: 15, 18: 17, 20: 19, 22: 21, 24: 23}
    inner_first = {
        0: ((3, 0, 0), (3, 1, 0)), 1: ((3, 2, 0), (3, 3, 0)), 2: ((1, 0, 0),), 3: ((2, 0, 0),),
        4: ((1, 1, 0), (0, 0, 0)), 6: ((1, 2, 0), (0, 1, 0)), 8: ((1, 3, 0), (0, 2, 0)),
        9: ((0, 0, 1), (0, 1, 1)), 11: ((0, 3, 0), (0, 2, 1), (0, 3, 1)),
        14: ((1, 0, 1), (1, 1, 1)), 15: ((1, 2, 1), (1, 3, 1)), 16: ((2, 0, 1), (2, 1, 0)), 17: ((2, 1, 1), (2, 2, 0)),
        18: ((2, 2, 1), (2, 3, 0)), 19: ((2, 3, 1), (3, 0, 1)), 20: ((3, 1, 1), (3, 2, 1)), 21: ((3, 3, 1),),
    }
    inner_second = {
        12: ((0, 0), (0, 1)), 13: ((0, 2), (0, 3)), 15: ((1, 0), (1, 1)), 16: ((1, 2), (1, 3)), 17: ((2, 0),),
        18: ((2, 1),), 19: ((2, 2),), 20: ((2, 3), (3, 0)), 21: ((3, 1), (3, 2)), 22: ((3, 3),),
    }

    def packed(plan, width):
        entries = {}
        for at, todo in plan.items():
            entries[at] = 0
            for k, (blk, part_of, *s) in enumerate(todo):
                number = blk * UNITS + part_of
                entries[at] += ((2 * number + s[0] if s else number) + 1) * width ** k
        return entries

    first_width, second_width = 8 * UNITS * 2, 8 * UNITS
    plans = (
        packed(outer_first, first_width), packed(inner_first, first_width),
        packed(outer_second, second_width), packed(inner_second, second_width),
    )

    for copy in local[4:]:
        copy.wait()

    @pl.when(outer)
    def _():
        table(mid, 0, to_mid).wait_recv()

    @pl.when(inner)
    def _():
        table(end, 0, to_end).wait_recv()
        table(end, 1, to_far).start()
        table(far_mid, 1, to_far).wait_recv()
        table(far_mid, 0, to_end).start()
        for b in (end, far_mid):
            columns[b] = wt[b].T

    def step(n, carry):
        @pl.when(n < head)
        def _():
            got_y(n)

        ahead = look(n, outer_pairs)

        @pl.when(outer)
        def _():
            @pl.when(n == PIECES)
            def _():
                for u in range(UNITS):
                    shared(mid, u)
                slim_rows(0)
                compact(0, to_mid).start()

            @pl.when(n < head)
            def _():
                outer_stream(n)

            @pl.when(ahead > 0)
            def _():
                outer_stream(ahead - 1)
                outer_stream(ahead)

        @pl.when(inner)
        def _():
            @pl.when(n < PIECES)
            def _():
                inner_end(n)

            @pl.when((n < head) | ((n >= head + 2) & (n < head + 6)))
            def _():
                inner_stream(jnp.where(n < head, n, n - 2))

            @pl.when(n == LEAD)
            def _():
                table(far_end, 1, to_far).wait_recv()
                table(far_end, 0, to_end).start()
                columns[far_end] = wt[far_end].T

        @pl.when(n == PIECES + 1)
        def _():
            got_x(0)
            got_x(1)

        @pl.when(outer)
        def _():
            @pl.when(n == head - 1)
            def _():
                table(far_end, 0, to_mid).wait_recv()
                table(far_mid, 0, to_mid).wait_recv()
                for b in (far_end, far_mid):
                    columns[b] = wt[b].T

        @pl.when(inner)
        def _():
            q = n - head - 2

            @pl.when((q >= 0) & (q < PIECES))
            def _():
                pass_on(far_end, q, to_far)

            @pl.when((q >= 3) & (q < PIECES + 3))
            def _():
                pass_on(end, q - 3, to_end)

            @pl.when((q >= PIECES) & (q < 2 * PIECES))
            def _():
                pass_on(far_mid, q - PIECES, to_far)

            @pl.when(q == PIECES + 1)
            def _():
                compact(0, to_end).wait_recv()
                acc[...] = acc[...] + widen(0)

            @pl.when(q >= PIECES + 2)
            def _():
                take_in(q - PIECES - 2)

        todo = jnp.where(outer, look(n, plans[0]), look(n, plans[1]))

        def first(v, left):
            code = left % first_width

            @pl.when(code > 0)
            def _():
                first_stage(code - 1)
            return left // first_width

        lax.fori_loop(0, 4, first, todo)

        @pl.when(n == jnp.where(outer, head - 1, head))
        def _():
            got_x(2)

        todo = jnp.where(outer, look(n, plans[2]), look(n, plans[3]))

        def second(v, left):
            pair = left % second_width

            @pl.when(pair > 0)
            def _():
                second_stage(pair - 1)
            return left // second_width

        lax.fori_loop(0, 2, second, todo)

        @pl.when(outer & (n == head + 3))
        def _():
            slim_rows(1)
        return carry

    lax.fori_loop(0, 4 * PIECES, step, 0)

    @pl.when(outer)
    def _():
        compact(1, to_mid).start()

    @pl.when(outer)
    def _():
        for q in range(PIECES):
            total(z, q, to_mid).wait_recv()
            at = span(q)
            out_ref[at] = (acc[at] + came[z, at].astype(f32)).astype(bf16)

    @pl.when(inner)
    def _():
        compact(1, to_end).wait_recv()
        out_ref[...] = (acc[...] + widen(1)).astype(bf16)

    swap(0, PIECES).wait_send()
    for m in range(3):
        send_y(m, 0, CUTS).wait_send()
        send_x(m, 0, g, CUTS).wait_send()

    def handed(count):
        at = hid.at[pl.ds(0, count), c]
        remote(at, at, hid_s, hid_r.at[0], mate).wait_send()

    def blocks_shared(blocks):
        for b in blocks:
            remote(x.at[b, c], x.at[b, c], half_s.at[b], half_r.at[b, 0], mate).wait_send()

    @pl.when(outer)
    def _():
        table(z, 0, to_mid).wait_send()
        remote(slim, slim_in, slim_s, slim_r.at[0], to_mid).wait_send()
        at = slim_hid.at[pl.ds(0, 2), c]
        remote(at, at, few_s, few_r.at[0], mate).wait_send()
        handed(6 * UNITS)
        gather_sent(z, 0, to_mid)
        for b in (far_end, far_mid):
            total_sent(b, to_mid)
        blocks_shared((mid, far_end, far_mid))

    @pl.when(inner)
    def _():
        handed(8 * UNITS)
        table(z, 0, to_end).wait_send()
        table(z, 1, to_far).wait_send()
        table(end, 1, to_far).wait_send()
        table(far_mid, 0, to_end).wait_send()
        table(far_end, 0, to_end).wait_send()
        for b in (z, far_mid, far_end):
            gather_sent(b, 0, to_end)
        for b in (z, end):
            gather_sent(b, 1, to_far)
        total_sent(end, to_end)
        for b in (far_mid, far_end):
            total_sent(b, to_far)
        blocks_shared((end, far_mid, far_end))


def line_form(tokens, norm_gain, expert_ids, route_weights, gate_weight, up_weight, down_weight):
    tok_rows, half = tokens.shape
    experts = lax.axis_size("ep")
    length = experts // COLS
    top = expert_ids.shape[1]
    cap = (3 * tok_rows * top + 2 * experts - 1) // (2 * experts)
    bf16, f32 = jnp.bfloat16, jnp.float32
    gate, up, down = gate_weight[0], up_weight[0], down_weight[0]
    dma, vmem = pltpu.SemaphoreType.DMA, pltpu.VMEM
    block = (length, tok_rows, half)
    pairs = UNITS * length
    bits = (length, PIECES)
    sems = [dma, dma((PIECES,)), dma((7,))]
    for send, recv in (
        ((3,), (3, CUTS)), ((3,), (3,)), ((2, length), bits), ((2, length), (length,)),
        ((length,), (length, UNITS)), ((), (pairs,)), ((), (2,)), ((length,), bits), ((), (2,)),
    ):
        sems += [dma(send) if send else dma, dma(recv)]
    return pl.pallas_call(
        functools.partial(line_kernel, length, cap),
        out_shape=vmem((tok_rows, half), bf16),
        in_specs=[pl.BlockSpec(memory_space=pl.ANY)] * 7,
        out_specs=pl.BlockSpec(memory_space=vmem),
        scratch_shapes=[
            vmem((tok_rows, half), bf16),
            vmem((2, 1, half), f32),
            vmem((top, tok_rows), jnp.int32),
            vmem((top, tok_rows), f32),
            vmem((tok_rows, half), bf16),
            vmem((length, 2, tok_rows, half), bf16),
            vmem((length, experts, tok_rows), f32),
            vmem((length, tok_rows, experts), f32),
            vmem((2,) + gate.shape, bf16),
            vmem((2,) + up.shape, bf16),
            vmem((2,) + down.shape, bf16),
            vmem((2 * pairs, 2, tok_rows // UNITS, gate.shape[1]), bf16),
            vmem((2, 2, cap, gate.shape[1]), bf16),
            vmem(block, bf16),
            vmem(block, bf16),
            vmem((2, cap, half), bf16),
            vmem((2, cap, half), bf16),
            vmem((tok_rows, half), f32),
        ]
        + sems,
        compiler_params=pltpu.CompilerParams(
            collective_id=0, has_side_effects=True, vmem_limit_bytes=58 * 1024 * 1024
        ),
    )(tokens, norm_gain.reshape(2, 1, half), expert_ids.T, route_weights.T, gate, up, down)


def solution(mesh):
    in_specs = (
        P(("grp", "ep"), "tp"),
        P(),
        P(("grp", "ep"), None),
        P(("grp", "ep"), None),
        P("ep", None, "tp"),
        P("ep", None, "tp"),
        P("ep", None, "tp"),
    )
    out_specs = P(("grp", "ep"), "tp")
    shape = mesh.shape

    def on_device(tokens, norm_gain, expert_ids, *rest):
        dense = shape["ep"] == 4 * COLS and shape["ep"] == 4 * expert_ids.shape[1]
        form = line_form if dense and shape["grp"] == 2 and shape["tp"] == 2 else sparse_form
        return form(tokens, norm_gain, expert_ids, *rest)

    return jax.shard_map(
        on_device, mesh=mesh, in_specs=in_specs, out_specs=out_specs, check_vma=False
    )
```

```python
import functools

import jax
import jax.numpy as jnp
from jax import lax
from jax.experimental import pallas as pl
from jax.experimental.pallas import tpu as pltpu
from jax.sharding import PartitionSpec as P

MESH = pl.DeviceIdType.MESH
COLS = 2
PIECES = 8
UNITS = 4
LEAD = 2
CUTS = 8


def normalize(rows, norm_gain):
    xf = rows.astype(jnp.float32)
    scale = lax.rsqrt(jnp.mean(xf * xf, axis=-1, keepdims=True) + 1e-06)
    return (xf * scale * norm_gain[None, :]).astype(jnp.bfloat16)


def sparse_form(tokens, norm_gain, expert_ids, route_weights, gate_weight, up_weight, down_weight):
    tok_rows, half = tokens.shape
    width = half * lax.axis_size("tp")
    experts = lax.axis_size("ep")
    top = expert_ids.shape[1]
    capacity = max(2, (3 * tok_rows * top + 2 * experts - 1) // (2 * experts))
    flat = expert_ids.reshape(-1)
    onehot = (flat[:, None] == jnp.arange(experts, dtype=jnp.int32)[None, :]).astype(jnp.int32)
    earlier = jnp.cumsum(onehot, axis=0) - onehot
    slot = jnp.sum(earlier * onehot, axis=-1)
    position = flat * capacity + slot
    owner = jnp.arange(flat.shape[0], dtype=jnp.int32) // top
    w_gate = gate_weight[0]
    w_up = up_weight[0]
    w_down = down_weight[0]
    send = jnp.zeros((experts * capacity, half), jnp.bfloat16).at[position].set(tokens[owner])
    send = send.reshape(experts, capacity, half)
    received = lax.all_to_all(send, "ep", split_axis=0, concat_axis=0, tiled=True)
    sources = received.shape[0]
    count = received.shape[1]
    whole_rows = lax.all_gather(received, "tp", axis=2, tiled=True)
    rows = normalize(whole_rows.reshape(sources * count, width), norm_gain)
    gate = jnp.dot(rows, w_gate, preferred_element_type=jnp.float32)
    upper = jnp.dot(rows, w_up, preferred_element_type=jnp.float32)
    hidden = (jax.nn.silu(gate) * upper).astype(jnp.bfloat16)
    result = jnp.dot(
        lax.all_gather(hidden, "tp", axis=1, tiled=True), w_down, preferred_element_type=jnp.float32
    )
    result = result.astype(jnp.bfloat16).reshape(sources, count, half)
    back = lax.all_to_all(result, "ep", split_axis=0, concat_axis=0, tiled=True)
    picked = back.reshape(experts * capacity, half)[position].astype(jnp.float32)
    picked = picked * route_weights.reshape(-1)[:, None]
    return jnp.sum(picked.reshape(tok_rows, top, half), axis=1).astype(jnp.bfloat16)


def line_kernel(
    length, cap, tok_ref, gain_in, ids_in, route_in, gate_in, up_in, down_in, out_ref,
    own, gain_ref, ids_ref, route_ref, raw, x, wt, columns, wg, wu, wd, hid, slim_hid, picked, slim_w, part, came, slim, slim_in, acc,
    swap_s, swap_r, loc, wy_s, wy_r, wx_s, wx_r, gat_s, gat_r, tab_s, tab_r,
    half_s, half_r, hid_s, hid_r, few_s, few_r, pick_s, pick_r, match_s, match_r, sum_s, sum_r, slim_s, slim_r,
):
    f32, bf16 = jnp.float32, jnp.bfloat16
    g, ep, c = lax.axis_index("grp"), lax.axis_index("ep"), lax.axis_index("tp")
    z, y = ep // COLS, ep % COLS
    last = length - 1
    flip = z >= length // 2
    end = jnp.where(flip, last, 0)
    mid = jnp.where(flip, last - 1, 1)
    far_mid, far_end = last - mid, last - end
    outer, inner = z == end, z == mid
    mate, across, beside = {"tp": 1 - c}, {"grp": 1 - g}, {"ep": z * COLS + 1 - y}
    to_end, to_mid, to_far = {"ep": end * COLS + y}, {"ep": mid * COLS + y}, {"ep": far_mid * COLS + y}
    rows, half = raw.shape
    piece = rows // PIECES
    unit = rows // UNITS
    per_unit = PIECES // UNITS
    wide = hid.shape[3]

    def remote(src, dst, ss, rs, dev):
        return pltpu.make_async_remote_copy(
            src_ref=src, dst_ref=dst, send_sem=ss, recv_sem=rs, device_id=dev, device_id_type=MESH
        )

    def span(q):
        return pl.ds(q * piece if isinstance(q, int) else pl.multiple_of(q * piece, piece), piece)

    barrier = pltpu.get_barrier_semaphore()
    for dev in (mate, across, beside):
        pl.semaphore_signal(barrier, inc=1, device_id=dev, device_id_type=MESH)

    @pl.when(outer)
    def _():
        pl.semaphore_signal(barrier, inc=1, device_id=to_mid, device_id_type=MESH)

    @pl.when(inner)
    def _():
        pl.semaphore_signal(barrier, inc=1, device_id=to_end, device_id_type=MESH)
        pl.semaphore_signal(barrier, inc=1, device_id=to_far, device_id_type=MESH)

    inputs = ((tok_ref, own), (gain_in, gain_ref), (ids_in, ids_ref), (route_in, route_ref))
    inputs += ((gate_in, wg.at[0]), (up_in, wu.at[0]), (down_in, wd.at[0]))
    local = [pltpu.make_async_copy(src, dst, loc.at[k]) for k, (src, dst) in enumerate(inputs)]
    for copy in local:
        copy.start()
    pl.semaphore_wait(barrier, jnp.where(outer, 4, 5))

    mats = ((gate_in, wg), (up_in, wu), (down_in, wd))

    columns_cut = down_in.shape[1] // CUTS

    def cut(m, portion, u, many=1):
        if m < 2:
            size = mats[m][0].shape[0] // (2 * CUTS)
            return (pl.ds(pl.multiple_of((portion * CUTS + u) * size, size), size * many), pl.ds(0, wide))
        first = pl.multiple_of((portion * (CUTS // 2) + u // 2) * columns_cut, columns_cut)
        if many == 1:
            return (pl.ds(pl.multiple_of(u % 2 * wide, wide), wide), pl.ds(first, columns_cut))
        return (pl.ds(0, 2 * wide), pl.ds(first, columns_cut * (many // 2)))

    def send_y(m, u, many=1):
        src, dst = mats[m]
        at = cut(m, g, u, many)
        return remote(src.at[at], dst.at[(1,) + at], wy_s.at[m], wy_r.at[m, u], beside)

    def send_x(m, u, portion, many=1):
        buf = mats[m][1].at[(1,) + cut(m, portion, u, many)]
        return remote(buf, buf, wx_s.at[m], wx_r.at[m if m < 2 else 2 + u // 2], across)

    for m in range(3):
        for u in range(CUTS):
            send_y(m, u).start()

    def swap(q, many=1):
        at = pl.ds(q * piece if isinstance(q, int) else pl.multiple_of(q * piece, piece), piece * many)
        return remote(own.at[at], raw.at[at], swap_s, swap_r.at[q], mate)

    local[0].wait()
    for q in range(PIECES):
        swap(q).start()
    for copy in local[1:4]:
        copy.wait()

    def gather(b, q, way, dev):
        at = x.at[b, c, span(q)]
        return remote(at, at, gat_s.at[way, b], gat_r.at[b, q], dev)

    def gather_sent(b, way, dev):
        remote(x.at[b, c], x.at[b, c], gat_s.at[way, b], gat_r.at[b, 0], dev).wait_send()

    def table(b, way, dev):
        return remote(wt.at[b], wt.at[b], tab_s.at[way, b], tab_r.at[b], dev)

    def share(b, q):
        at = x.at[b, c, span(q)]
        return remote(at, at, half_s.at[b], half_r.at[b, q // per_unit], mate)

    def shared(b, part_of):
        at = x.at[b, 1 - c, rows_of(part_of)]
        remote(at, at, half_s.at[b], half_r.at[b, part_of], mate).wait_recv()

    def rows_of(part_of):
        return pl.ds(part_of * unit if isinstance(part_of, int) else pl.multiple_of(part_of * unit, unit), unit)

    def total(b, q, dev):
        return remote(part.at[b, span(q)], came.at[b, span(q)], sum_s.at[b], sum_r.at[b, q], dev)

    def total_sent(b, dev):
        remote(part.at[b], came.at[b], sum_s.at[b], sum_r.at[b, 0], dev).wait_send()

    def compact(s, dev):
        return remote(slim.at[s], slim_in.at[s], slim_s, slim_r.at[s], dev)

    def hand(pair, s):
        at = hid.at[2 * pair + s, c]
        return remote(at, at, hid_s, hid_r.at[pair], mate)

    def chosen_rows(s, dev):
        at = picked.at[s, c]
        return remote(at, at, pick_s, pick_r.at[s], dev)

    def match(s, side):
        at = picked.at[s, side]
        return remote(at, at, match_s, match_r.at[s], mate)

    def compact_columns(at):
        return remote(slim.at[1, :, at], slim_in.at[1, :, at], slim_s, slim_r.at[1], to_mid)

    def hand_few(s, side):
        at = slim_hid.at[s, side]
        return remote(at, at, few_s, few_r.at[s], mate)

    named = lax.broadcasted_iota(jnp.int32, wt.shape[1:], 0)
    routes = None
    for k in range(ids_ref.shape[0]):
        term = jnp.where(named == ids_ref[pl.ds(k, 1)], route_ref[pl.ds(k, 1)], 0.0)
        routes = term if routes is None else routes + term
    wt[z] = routes

    @pl.when(outer)
    def _():
        table(z, 0, to_mid).start()

    @pl.when(inner)
    def _():
        table(z, 0, to_end).start()
        table(z, 1, to_far).start()

    def norm(q, carry):
        swap(q).wait_recv()
        at = span(q)
        a = own[at].astype(f32)
        b = raw[at].astype(f32)
        total_sq = jnp.sum(a * a, axis=-1, keepdims=True) + jnp.sum(b * b, axis=-1, keepdims=True)
        scale = lax.rsqrt(total_sq / (2 * half) + 1e-06)
        x[z, c, at] = (a * scale * gain_ref[c]).astype(bf16)
        x[z, 1 - c, at] = (b * scale * gain_ref[1 - c]).astype(bf16)

        @pl.when(outer)
        def _():
            gather(z, q, 0, to_mid).start()

        @pl.when(inner)
        def _():
            @pl.when(q < LEAD)
            def _():
                gather(z, q, 1, to_far).start()
        return carry

    lax.fori_loop(0, PIECES, norm, 0)
    columns[z] = wt[z].T

    def got_y(n):
        for m in range(3):
            @pl.when(n // (CUTS // 2) == m)
            def _():
                for v in range(2):
                    u = n % (CUTS // 2) * 2 + v
                    send_y(m, u).wait_recv()
                    send_x(m, u, g).start()

    def got_x(m):
        send_x(m, 0, 1 - g, CUTS).wait_recv()

    def got_columns(k):
        send_x(2, 2 * k, 1 - g, 2).wait_recv()

    def outer_stream(j):
        b = jnp.where(j < PIECES, far_end, far_mid)
        q = j % PIECES
        gather(b, q, 0, to_mid).wait_recv()
        share(b, q).start()

    def inner_stream(j):
        lead = j < LEAD
        turn = (j >= LEAD) & (j < LEAD + PIECES)
        b = jnp.where(turn, far_end, far_mid)
        q = jnp.where(lead, j, jnp.where(turn, j - LEAD, j - PIECES))
        gather(b, q, 1, to_far).wait_recv()
        share(b, q).start()

        @pl.when(j >= LEAD)
        def _():
            gather(b, q, 0, to_end).start()

        @pl.when(j == LEAD + PIECES - 1)
        def _():
            for early in range(LEAD):
                gather(far_mid, early, 0, to_end).start()

    def inner_end(q):
        gather(end, q, 0, to_end).wait_recv()
        share(end, q).start()
        gather(end, q, 1, to_far).start()

        @pl.when(q == PIECES - 1)
        def _():
            for late in range(LEAD, PIECES):
                gather(z, late, 1, to_far).start()

    def pick(table_rows, e):
        lane = lax.broadcasted_iota(jnp.int32, table_rows.shape, 0)
        return jnp.sum(jnp.where(lane == e, table_rows, 0.0), axis=0, keepdims=True)

    def selection(b, e):
        weights = wt[b]
        chosen = jnp.where(weights > 0.0, 1.0, 0.0)
        above = lax.broadcasted_iota(jnp.int32, (rows, rows), 0)
        along = lax.broadcasted_iota(jnp.int32, (rows, rows), 1)
        before = jnp.where(above < along, 1.0, 0.0).astype(bf16)
        rank = jnp.dot(chosen.astype(bf16), before, preferred_element_type=f32)
        place = pick(jnp.where(chosen > 0.0, rank, -1.0), e)
        slot = lax.broadcasted_iota(jnp.int32, (cap, rows), 0).astype(f32)
        return jnp.where(slot == place, 1.0, 0.0), pick(weights, e)

    def hidden_half(first, second, s):
        both = []
        for w in (wg, wu):
            both.append(
                jnp.dot(first, w[s, :half], preferred_element_type=f32)
                + jnp.dot(second, w[s, half:], preferred_element_type=f32)
            )
        gate, upper = both
        return (gate * (0.5 * (1.0 + jnp.tanh(0.5 * gate))) * upper).astype(bf16)

    def lowered(left, right, s):
        return jnp.dot(left, wd[s, :wide], preferred_element_type=f32) + jnp.dot(
            right, wd[s, wide:], preferred_element_type=f32
        )

    def pick_rows(s):
        mark, _ = selection(mid, end * COLS + (y if s == 0 else 1 - y))
        picked[s, c] = jnp.dot(mark.astype(bf16), x[mid, c], preferred_element_type=f32).astype(bf16)
        chosen_rows(s, to_end).start()

    def got_rows(s):
        chosen_rows(s, to_mid).wait_recv()
        match(s, c).start()

    def slim_first(s):
        match(s, 1 - c).wait_recv()
        slim_hid[s, c] = hidden_half(picked[s, 0], picked[s, 1], s)
        hand_few(s, c).start()

    def slim_weight(s):
        mark, weight_row = selection(mid, end * COLS + (y if s == 0 else 1 - y))
        return jnp.sum(mark * weight_row, axis=1, keepdims=True)

    def slim_rows():
        slim_first(0)
        weight = slim_weight(0)
        hand_few(0, 1 - c).wait_recv()
        slim[0] = (lowered(slim_hid[0, 0], slim_hid[0, 1], 0) * weight).astype(bf16)
        compact(0, to_mid).start()

    def columns_at(k, portion):
        return pl.ds(pl.multiple_of((portion * (CUTS // 2) + k) * columns_cut, columns_cut), columns_cut)

    def slim_columns(k):
        for portion in (g, 1 - g):
            at = columns_at(k, portion)
            got = jnp.dot(slim_hid[1, 0], wd[1, :wide, at], preferred_element_type=f32) + jnp.dot(
                slim_hid[1, 1], wd[1, wide:, at], preferred_element_type=f32
            )
            slim[1, :, at] = (got * slim_w[...]).astype(bf16)

    def send_columns(k):
        for portion in (g, 1 - g):
            compact_columns(columns_at(k, portion)).start()

    def widen(s):
        mark, _ = selection(mid, end * COLS + (y if s == 0 else 1 - y))
        ones = mark.astype(bf16)
        return lax.dot_general(ones, slim_in[s], (((0,), (0,)), ((), ())), preferred_element_type=f32)

    def block_of(k):
        return jnp.where(k == 0, far_end, jnp.where(k == 1, end, jnp.where(k == 2, far_mid, mid)))

    def first_stage(code):
        pair, s = code // 2, code % 2
        b, part_of = block_of(pair // UNITS), pair % UNITS

        @pl.when((s == 0) & (b != z))
        def _():
            shared(b, part_of)

        at = rows_of(part_of)
        hid[code, c] = hidden_half(x[b, 0, at], x[b, 1, at], s)
        hand(pair, s).start()

    def second_stage(pair):
        b, part_of = block_of(pair // UNITS), pair % UNITS
        at = rows_of(part_of)
        mine = columns[b, at]
        lane = lax.broadcasted_iota(jnp.int32, mine.shape, 1)
        both = hid.at[pl.ds(2 * pair, 2), 1 - c]
        remote(both, both, hid_s, hid_r.at[pair], mate).wait_recv()
        sums = None
        for s in range(2):
            expert = z * COLS + (y if s == 0 else 1 - y)
            weight = jnp.sum(jnp.where(lane == expert, mine, 0.0), axis=1, keepdims=True)
            got = lowered(hid[2 * pair + s, 0], hid[2 * pair + s, 1], s) * weight
            sums = got if sums is None else sums + got

        @pl.when(b == z)
        def _():
            acc[at] = sums

        @pl.when(b != z)
        def _():
            part[b, at] = sums.astype(bf16)

        @pl.when(outer & (b != z))
        def _():
            for n in range(per_unit):
                total(b, part_of * per_unit + n, to_mid).start()

    def pass_on(b, q, dev):
        total(b, q, dev).wait_recv()
        at = span(q)
        part[b, at] = (part[b, at].astype(f32) + came[b, at].astype(f32)).astype(bf16)
        total(b, q, dev).start()

    def take_in(q):
        total(z, q, to_far).wait_recv()
        at = span(q)
        acc[at] = acc[at] + came[z, at].astype(f32)

    def look(n, entries):
        value = 0
        for at, entry in entries.items():
            value = jnp.where(n == at, entry, value)
        return value

    head = 3 * CUTS // 2
    outer_first = {
        0: ((1, 0, 0), (1, 1, 0)), 1: ((1, 2, 0), (1, 3, 0)), 10: ((0, 0, 0), (0, 0, 1)), 11: ((0, 1, 0), (0, 1, 1)),
        13: ((0, 2, 0), (0, 2, 1)), 14: ((1, 0, 1), (1, 1, 1)), 15: ((0, 3, 0), (0, 3, 1)), 16: ((1, 2, 1), (1, 3, 1)),
        19: ((2, 0, 0), (2, 0, 1)), 21: ((2, 1, 0), (2, 1, 1)), 23: ((2, 2, 0), (2, 2, 1)), 25: ((2, 3, 0), (2, 3, 1)),
    }
    outer_second = {
        12: ((0, 0), (0, 1)), 13: ((0, 2),), 15: ((0, 3),), 16: ((1, 0), (1, 1)), 17: ((1, 2), (1, 3)),
        19: ((2, 0),), 21: ((2, 1),), 23: ((2, 2),), 25: ((2, 3),),
    }
    outer_pairs = {13: 5, 15: 7, 18: 9, 20: 11, 22: 13, 24: 15}
    inner_first = {
        0: ((3, 0, 0), (3, 1, 0)), 1: ((3, 2, 0), (3, 3, 0)), 2: ((1, 0, 0),), 3: ((2, 0, 0),),
        4: ((1, 1, 0), (0, 0, 0)), 6: ((1, 2, 0), (0, 1, 0)), 8: ((1, 3, 0), (0, 2, 0)),
        9: ((0, 0, 1), (0, 1, 1)), 11: ((0, 3, 0), (0, 2, 1), (0, 3, 1)),
        14: ((1, 0, 1), (1, 1, 1)), 15: ((1, 2, 1), (1, 3, 1)), 16: ((2, 0, 1), (2, 1, 0)), 17: ((2, 1, 1), (2, 2, 0)),
        18: ((2, 2, 1), (2, 3, 0)), 19: ((2, 3, 1), (3, 0, 1)), 20: ((3, 1, 1), (3, 2, 1)), 21: ((3, 3, 1),),
    }
    inner_second = {
        12: ((0, 0), (0, 1)), 13: ((0, 2), (0, 3)), 15: ((1, 0), (1, 1)), 16: ((1, 2), (1, 3)), 17: ((2, 0),),
        18: ((2, 1),), 19: ((2, 2),), 20: ((2, 3), (3, 0)), 21: ((3, 1), (3, 2)), 22: ((3, 3),),
    }

    def packed(plan, width):
        entries = {}
        for at, todo in plan.items():
            entries[at] = 0
            for k, (blk, part_of, *s) in enumerate(todo):
                number = blk * UNITS + part_of
                entries[at] += ((2 * number + s[0] if s else number) + 1) * width ** k
        return entries

    first_width, second_width = 8 * UNITS * 2, 8 * UNITS
    plans = (
        packed(outer_first, first_width), packed(inner_first, first_width),
        packed(outer_second, second_width), packed(inner_second, second_width),
    )

    for copy in local[4:]:
        copy.wait()

    @pl.when(outer)
    def _():
        table(mid, 0, to_mid).wait_recv()

    @pl.when(inner)
    def _():
        for s in range(2):
            pick_rows(s)
        table(end, 0, to_end).wait_recv()
        table(end, 1, to_far).start()
        table(far_mid, 1, to_far).wait_recv()
        table(far_mid, 0, to_end).start()
        for b in (end, far_mid):
            columns[b] = wt[b].T

    def step(n, carry):
        @pl.when(n < head)
        def _():
            got_y(n)

        ahead = look(n, outer_pairs)

        @pl.when(outer)
        def _():
            @pl.when(n == PIECES // 2)
            def _():
                got_rows(0)
                slim_rows()

            @pl.when(n == PIECES - 1)
            def _():
                got_rows(1)
                slim_w[...] = jnp.broadcast_to(slim_weight(1), slim_w.shape)

            @pl.when((n >= PIECES) & (n < head))
            def _():
                outer_stream(n - PIECES)

            @pl.when(ahead > 0)
            def _():
                outer_stream(ahead - 1)
                outer_stream(ahead)

        @pl.when(inner)
        def _():
            @pl.when(n < PIECES)
            def _():
                inner_end(n)

            @pl.when((n < head) | ((n >= head + 2) & (n < head + 6)))
            def _():
                inner_stream(jnp.where(n < head, n, n - 2))

            @pl.when(n == LEAD)
            def _():
                table(far_end, 1, to_far).wait_recv()
                table(far_end, 0, to_end).start()
                columns[far_end] = wt[far_end].T

        @pl.when(n == PIECES + 1)
        def _():
            got_x(0)
            got_x(1)

        @pl.when(outer)
        def _():
            @pl.when(n == PIECES + 1)
            def _():
                slim_first(1)

            for k in range(CUTS // 2):
                @pl.when(n == min(head, PIECES + 2 + k))
                def _():
                    got_columns(k)
                    if k == 0:
                        hand_few(1, 1 - c).wait_recv()
                    if k < CUTS // 2 - 1:
                        slim_columns(k)
                        send_columns(k)

            @pl.when(n == head + 2)
            def _():
                slim_columns(CUTS // 2 - 1)

        @pl.when(outer)
        def _():
            @pl.when(n == head - 1)
            def _():
                table(far_end, 0, to_mid).wait_recv()
                table(far_mid, 0, to_mid).wait_recv()
                for b in (far_end, far_mid):
                    columns[b] = wt[b].T

        @pl.when(inner)
        def _():
            q = n - head - 2

            @pl.when((q >= 0) & (q < PIECES))
            def _():
                pass_on(far_end, q, to_far)

            @pl.when((q >= 3) & (q < PIECES + 3))
            def _():
                pass_on(end, q - 3, to_end)

            @pl.when((q >= PIECES) & (q < 2 * PIECES))
            def _():
                pass_on(far_mid, q - PIECES, to_far)

            @pl.when(q == PIECES + 1)
            def _():
                compact(0, to_end).wait_recv()
                acc[...] = acc[...] + widen(0)

            @pl.when(n == 4 * PIECES - 1)
            def _():
                compact(1, to_end).wait_recv()
                acc[...] = acc[...] + widen(1)

            @pl.when(q >= PIECES + 2)
            def _():
                take_in(q - PIECES - 2)

        todo = jnp.where(outer, look(n, plans[0]), look(n, plans[1]))

        def first(v, left):
            code = left % first_width

            @pl.when(code > 0)
            def _():
                first_stage(code - 1)
            return left // first_width

        lax.fori_loop(0, 4, first, todo)

        @pl.when(inner & (n == head))
        def _():
            for k in range(CUTS // 2):
                got_columns(k)

        todo = jnp.where(outer, look(n, plans[2]), look(n, plans[3]))

        def second(v, left):
            pair = left % second_width

            @pl.when(pair > 0)
            def _():
                second_stage(pair - 1)
            return left // second_width

        lax.fori_loop(0, 2, second, todo)

        @pl.when(outer & (n == 3 * PIECES + 2))
        def _():
            send_columns(CUTS // 2 - 1)
        return carry

    lax.fori_loop(0, 4 * PIECES, step, 0)

    @pl.when(outer)
    def _():
        for q in range(PIECES):
            total(z, q, to_mid).wait_recv()
            at = span(q)
            out_ref[at] = (acc[at] + came[z, at].astype(f32)).astype(bf16)

    @pl.when(inner)
    def _():
        out_ref[...] = acc[...].astype(bf16)

    swap(0, PIECES).wait_send()
    for m in range(3):
        send_y(m, 0, CUTS).wait_send()
        send_x(m, 0, g, CUTS).wait_send()

    def handed(count):
        at = hid.at[pl.ds(0, count), c]
        remote(at, at, hid_s, hid_r.at[0], mate).wait_send()

    def blocks_shared(blocks):
        for b in blocks:
            remote(x.at[b, c], x.at[b, c], half_s.at[b], half_r.at[b, 0], mate).wait_send()

    @pl.when(outer)
    def _():
        table(z, 0, to_mid).wait_send()
        remote(slim, slim_in, slim_s, slim_r.at[0], to_mid).wait_send()
        at = slim_hid.at[pl.ds(0, 2), c]
        remote(at, at, few_s, few_r.at[0], mate).wait_send()
        handed(6 * UNITS)
        at = picked.at[pl.ds(0, 2), c]
        remote(at, at, match_s, match_r.at[0], mate).wait_send()
        gather_sent(z, 0, to_mid)
        for b in (far_end, far_mid):
            total_sent(b, to_mid)
        blocks_shared((far_end, far_mid))

    @pl.when(inner)
    def _():
        handed(8 * UNITS)
        table(z, 0, to_end).wait_send()
        table(z, 1, to_far).wait_send()
        table(end, 1, to_far).wait_send()
        table(far_mid, 0, to_end).wait_send()
        table(far_end, 0, to_end).wait_send()
        at = picked.at[pl.ds(0, 2), c]
        remote(at, at, pick_s, pick_r.at[0], to_end).wait_send()
        for b in (far_mid, far_end):
            gather_sent(b, 0, to_end)
        for b in (z, end):
            gather_sent(b, 1, to_far)
        total_sent(end, to_end)
        for b in (far_mid, far_end):
            total_sent(b, to_far)
        blocks_shared((end, far_mid, far_end))


def line_form(tokens, norm_gain, expert_ids, route_weights, gate_weight, up_weight, down_weight):
    tok_rows, half = tokens.shape
    experts = lax.axis_size("ep")
    length = experts // COLS
    top = expert_ids.shape[1]
    cap = (3 * tok_rows * top + 2 * experts - 1) // (2 * experts)
    bf16, f32 = jnp.bfloat16, jnp.float32
    gate, up, down = gate_weight[0], up_weight[0], down_weight[0]
    dma, vmem = pltpu.SemaphoreType.DMA, pltpu.VMEM
    block = (length, tok_rows, half)
    pairs = UNITS * length
    bits = (length, PIECES)
    sems = [dma, dma((PIECES,)), dma((7,))]
    for send, recv in (
        ((3,), (3, CUTS)), ((3,), (2 + CUTS // 2,)), ((2, length), bits), ((2, length), (length,)),
        ((length,), (length, UNITS)), ((), (pairs,)), ((), (2,)), ((), (2,)), ((), (2,)), ((length,), bits), ((), (2,)),
    ):
        sems += [dma(send) if send else dma, dma(recv)]
    return pl.pallas_call(
        functools.partial(line_kernel, length, cap),
        out_shape=vmem((tok_rows, half), bf16),
        in_specs=[pl.BlockSpec(memory_space=pl.ANY)] * 7,
        out_specs=pl.BlockSpec(memory_space=vmem),
        scratch_shapes=[
            vmem((tok_rows, half), bf16),
            vmem((2, 1, half), f32),
            vmem((top, tok_rows), jnp.int32),
            vmem((top, tok_rows), f32),
            vmem((tok_rows, half), bf16),
            vmem((length, 2, tok_rows, half), bf16),
            vmem((length, experts, tok_rows), f32),
            vmem((length, tok_rows, experts), f32),
            vmem((2,) + gate.shape, bf16),
            vmem((2,) + up.shape, bf16),
            vmem((2,) + down.shape, bf16),
            vmem((2 * pairs, 2, tok_rows // UNITS, gate.shape[1]), bf16),
            vmem((2, 2, cap, gate.shape[1]), bf16),
            vmem((2, 2, cap, half), bf16),
            vmem((cap, half // CUTS), f32),
            vmem(block, bf16),
            vmem(block, bf16),
            vmem((2, cap, half), bf16),
            vmem((2, cap, half), bf16),
            vmem((tok_rows, half), f32),
        ]
        + sems,
        compiler_params=pltpu.CompilerParams(
            collective_id=0, has_side_effects=True, vmem_limit_bytes=58 * 1024 * 1024
        ),
    )(tokens, norm_gain.reshape(2, 1, half), expert_ids.T, route_weights.T, gate, up, down)


def solution(mesh):
    in_specs = (
        P(("grp", "ep"), "tp"),
        P(),
        P(("grp", "ep"), None),
        P(("grp", "ep"), None),
        P("ep", None, "tp"),
        P("ep", None, "tp"),
        P("ep", None, "tp"),
    )
    out_specs = P(("grp", "ep"), "tp")
    shape = mesh.shape

    def on_device(tokens, norm_gain, expert_ids, *rest):
        dense = shape["ep"] == 4 * COLS and shape["ep"] == 4 * expert_ids.shape[1]
        form = line_form if dense and shape["grp"] == 2 and shape["tp"] == 2 else sparse_form
        return form(tokens, norm_gain, expert_ids, *rest)

    return jax.shard_map(
        on_device, mesh=mesh, in_specs=in_specs, out_specs=out_specs, check_vma=False
    )
```

```python
import functools

import jax
import jax.numpy as jnp
from jax import lax
from jax.experimental import pallas as pl
from jax.experimental.pallas import tpu as pltpu
from jax.sharding import PartitionSpec as P

MESH = pl.DeviceIdType.MESH
COLS = 2
PIECES = 8
UNITS = 4
LEAD = 2
SPLIT = 2
CUTS = 8


def normalize(rows, norm_gain):
    xf = rows.astype(jnp.float32)
    scale = lax.rsqrt(jnp.mean(xf * xf, axis=-1, keepdims=True) + 1e-06)
    return (xf * scale * norm_gain[None, :]).astype(jnp.bfloat16)


def sparse_form(tokens, norm_gain, expert_ids, route_weights, gate_weight, up_weight, down_weight):
    tok_rows, half = tokens.shape
    width = half * lax.axis_size("tp")
    experts = lax.axis_size("ep")
    top = expert_ids.shape[1]
    capacity = max(2, (3 * tok_rows * top + 2 * experts - 1) // (2 * experts))
    flat = expert_ids.reshape(-1)
    onehot = (flat[:, None] == jnp.arange(experts, dtype=jnp.int32)[None, :]).astype(jnp.int32)
    earlier = jnp.cumsum(onehot, axis=0) - onehot
    slot = jnp.sum(earlier * onehot, axis=-1)
    position = flat * capacity + slot
    owner = jnp.arange(flat.shape[0], dtype=jnp.int32) // top
    w_gate = gate_weight[0]
    w_up = up_weight[0]
    w_down = down_weight[0]
    send = jnp.zeros((experts * capacity, half), jnp.bfloat16).at[position].set(tokens[owner])
    send = send.reshape(experts, capacity, half)
    received = lax.all_to_all(send, "ep", split_axis=0, concat_axis=0, tiled=True)
    sources = received.shape[0]
    count = received.shape[1]
    whole_rows = lax.all_gather(received, "tp", axis=2, tiled=True)
    rows = normalize(whole_rows.reshape(sources * count, width), norm_gain)
    gate = jnp.dot(rows, w_gate, preferred_element_type=jnp.float32)
    upper = jnp.dot(rows, w_up, preferred_element_type=jnp.float32)
    hidden = (jax.nn.silu(gate) * upper).astype(jnp.bfloat16)
    result = jnp.dot(
        lax.all_gather(hidden, "tp", axis=1, tiled=True), w_down, preferred_element_type=jnp.float32
    )
    result = result.astype(jnp.bfloat16).reshape(sources, count, half)
    back = lax.all_to_all(result, "ep", split_axis=0, concat_axis=0, tiled=True)
    picked = back.reshape(experts * capacity, half)[position].astype(jnp.float32)
    picked = picked * route_weights.reshape(-1)[:, None]
    return jnp.sum(picked.reshape(tok_rows, top, half), axis=1).astype(jnp.bfloat16)


def line_kernel(
    length, cap, tok_ref, gain_in, ids_in, route_in, gate_in, up_in, down_in, out_ref,
    own, gain_ref, ids_ref, route_ref, raw, x, xn, wt, columns, wg, wu, wd, hid, slim_hid, picked, slim_w, part, came, slim, slim_in, acc,
    swap_s, swap_r, loc, wy_s, wy_r, wx_s, wx_r, gat_s, gat_r, tab_s, tab_r,
    half_s, half_r, hid_s, hid_r, few_s, few_r, pick_s, pick_r, match_s, match_r, sum_s, sum_r, slim_s, slim_r,
):
    f32, bf16 = jnp.float32, jnp.bfloat16
    g, ep, c = lax.axis_index("grp"), lax.axis_index("ep"), lax.axis_index("tp")
    z, y = ep // COLS, ep % COLS
    last = length - 1
    flip = z >= length // 2
    end = jnp.where(flip, last, 0)
    mid = jnp.where(flip, last - 1, 1)
    far_mid, far_end = last - mid, last - end
    outer, inner = z == end, z == mid
    mate, across, beside = {"tp": 1 - c}, {"grp": 1 - g}, {"ep": z * COLS + 1 - y}
    to_end, to_mid, to_far = {"ep": end * COLS + y}, {"ep": mid * COLS + y}, {"ep": far_mid * COLS + y}
    rows, half = raw.shape
    piece = rows // PIECES
    unit = rows // UNITS
    per_unit = PIECES // UNITS
    wide = hid.shape[3]

    def remote(src, dst, ss, rs, dev):
        return pltpu.make_async_remote_copy(
            src_ref=src, dst_ref=dst, send_sem=ss, recv_sem=rs, device_id=dev, device_id_type=MESH
        )

    def span(q):
        return pl.ds(q * piece if isinstance(q, int) else pl.multiple_of(q * piece, piece), piece)

    barrier = pltpu.get_barrier_semaphore()
    for dev in (mate, across, beside):
        pl.semaphore_signal(barrier, inc=1, device_id=dev, device_id_type=MESH)

    @pl.when(outer)
    def _():
        pl.semaphore_signal(barrier, inc=1, device_id=to_mid, device_id_type=MESH)

    @pl.when(inner)
    def _():
        pl.semaphore_signal(barrier, inc=1, device_id=to_end, device_id_type=MESH)
        pl.semaphore_signal(barrier, inc=1, device_id=to_far, device_id_type=MESH)

    inputs = ((tok_ref, own), (gain_in, gain_ref), (ids_in, ids_ref), (route_in, route_ref))
    inputs += ((gate_in, wg.at[0]), (up_in, wu.at[0]), (down_in, wd.at[0]))
    local = [pltpu.make_async_copy(src, dst, loc.at[k]) for k, (src, dst) in enumerate(inputs)]
    for copy in local:
        copy.start()
    pl.semaphore_wait(barrier, jnp.where(outer, 4, 5))

    mats = ((gate_in, wg), (up_in, wu), (down_in, wd))

    columns_cut = down_in.shape[1] // CUTS

    def cut(m, portion, u, many=1):
        if m < 2:
            size = mats[m][0].shape[0] // (2 * CUTS)
            return (pl.ds(pl.multiple_of((portion * CUTS + u) * size, size), size * many), pl.ds(0, wide))
        first = pl.multiple_of((portion * (CUTS // 2) + u // 2) * columns_cut, columns_cut)
        if many == 1:
            return (pl.ds(pl.multiple_of(u % 2 * wide, wide), wide), pl.ds(first, columns_cut))
        return (pl.ds(0, 2 * wide), pl.ds(first, columns_cut * (many // 2)))

    def send_y(m, u, many=1):
        dst = mats[m][1]
        at = cut(m, g, u, many)
        return remote(dst.at[(0,) + at], dst.at[(1,) + at], wy_s.at[m], wy_r.at[m, u], beside)

    def send_extra():
        at = cut(2, 1 - g, CUTS - 2, 2)
        return remote(
            wd.at[(0,) + at], wd.at[(1,) + at], wy_s.at[3], wx_r.at[1 + CUTS // 2], beside
        )

    def send_x(m, u, portion, many=1):
        buf = mats[m][1].at[(1,) + cut(m, portion, u, many)]
        return remote(buf, buf, wx_s.at[m], wx_r.at[m if m < 2 else 2 + u // 2], across)

    def swap(q, many=1):
        at = pl.ds(q * piece if isinstance(q, int) else pl.multiple_of(q * piece, piece), piece * many)
        return remote(own.at[at], raw.at[at], swap_s, swap_r.at[q], mate)

    def gather(b, q, way, dev, src=None):
        at = x.at[b, c, span(q)]
        return remote(at if src is None else src.at[span(q)], at, gat_s.at[way, b], gat_r.at[b, q], dev)

    for copy in local[2:4]:
        copy.wait()
    def table(b, way, dev):
        return remote(wt.at[b], wt.at[b], tab_s.at[way, b], tab_r.at[b], dev)

    named = lax.broadcasted_iota(jnp.int32, wt.shape[1:], 0)
    routes = None
    for k in range(ids_ref.shape[0]):
        term = jnp.where(named == ids_ref[pl.ds(k, 1)], route_ref[pl.ds(k, 1)], 0.0)
        routes = term if routes is None else routes + term
    wt[z] = routes

    @pl.when(outer)
    def _():
        table(z, 0, to_mid).start()

    @pl.when(inner)
    def _():
        table(z, 0, to_end).start()
        table(z, 1, to_far).start()

    local[0].wait()

    @pl.when(outer)
    def _():
        for q in range(PIECES):
            gather(z, q, 0, to_mid, own).start()

    @pl.when(inner)
    def _():
        for q in range(LEAD):
            gather(z, q, 1, to_far, own).start()

    for q in range(PIECES):
        swap(q).start()
    for m in range(3):
        local[4 + m].wait()
        for u in range(CUTS):
            send_y(m, u).start()
    send_extra().start()
    local[1].wait()

    def gather_sent(b, way, dev):
        remote(x.at[b, c], x.at[b, c], gat_s.at[way, b], gat_r.at[b, 0], dev).wait_send()

    def share(b, q):
        at = x.at[b, c, span(q)]
        return remote(at, at, half_s.at[b], half_r.at[b, q // per_unit], mate)

    def shared(b, part_of):
        at = x.at[b, 1 - c, rows_of(part_of)]
        remote(at, at, half_s.at[b], half_r.at[b, part_of], mate).wait_recv()

    def rows_of(part_of):
        return pl.ds(part_of * unit if isinstance(part_of, int) else pl.multiple_of(part_of * unit, unit), unit)

    def thin(r):
        size = piece // SPLIT
        return pl.ds(r * size if isinstance(r, int) else pl.multiple_of(r * size, size), size)

    def total(b, q, dev):
        return remote(part.at[b, thin(q)], came.at[b, thin(q)], sum_s.at[b], sum_r.at[b, q], dev)

    def total_sent(b, dev):
        remote(part.at[b], came.at[b], sum_s.at[b], sum_r.at[b, 0], dev).wait_send()

    def compact(s, dev):
        return remote(slim.at[s], slim_in.at[s], slim_s, slim_r.at[s], dev)

    def hand(pair, s):
        at = hid.at[2 * pair + s, c]
        return remote(at, at, hid_s, hid_r.at[pair], mate)

    def chosen_rows(s, dev):
        at = picked.at[s, c]
        return remote(at, at, pick_s, pick_r.at[s], dev)

    def match(s, side):
        at = picked.at[s, side]
        return remote(at, at, match_s, match_r.at[s], mate)

    def compact_columns(at):
        return remote(slim.at[1, :, at], slim_in.at[1, :, at], slim_s, slim_r.at[1], to_mid)

    def hand_few(s, side):
        at = slim_hid.at[s, side]
        return remote(at, at, few_s, few_r.at[s], mate)

    def normed(b, at, first, second):
        a, d = first.astype(f32), second.astype(f32)
        squares = jnp.sum(a * a, axis=-1, keepdims=True) + jnp.sum(d * d, axis=-1, keepdims=True)
        scale = lax.rsqrt(squares / (2 * half) + 1e-06)
        xn[b, 0, at] = (a * scale * gain_ref[0]).astype(bf16)
        xn[b, 1, at] = (d * scale * gain_ref[1]).astype(bf16)

    def norm(q, carry):
        swap(q).wait_recv()
        at = span(q)
        mine, other = own[at], raw[at]
        normed(z, at, jnp.where(c == 0, mine, other), jnp.where(c == 0, other, mine))
        return carry

    lax.fori_loop(0, PIECES, norm, 0)
    columns[z] = wt[z].T

    def got_y(n):
        for m in range(3):
            @pl.when(n // (CUTS // 2) == m)
            def _():
                for v in range(2):
                    u = n % (CUTS // 2) * 2 + v
                    send_y(m, u).wait_recv()

                    @pl.when((m < 2) | (u < CUTS - 2))
                    def _():
                        send_x(m, u, g).start()

    def got_x(m):
        send_x(m, 0, 1 - g, CUTS).wait_recv()

    def got_columns(k):
        if k == CUTS // 2 - 1:
            send_extra().wait_recv()
        else:
            send_x(2, 2 * k, 1 - g, 2).wait_recv()

    def outer_stream(j):
        b = jnp.where(j < PIECES, far_end, far_mid)
        q = j % PIECES
        gather(b, q, 0, to_mid).wait_recv()
        share(b, q).start()

    def inner_stream(j):
        lead = j < LEAD
        turn = (j >= LEAD) & (j < LEAD + PIECES)
        b = jnp.where(turn, far_end, far_mid)
        q = jnp.where(lead, j, jnp.where(turn, j - LEAD, j - PIECES))
        gather(b, q, 1, to_far).wait_recv()
        share(b, q).start()

        @pl.when(j >= LEAD)
        def _():
            gather(b, q, 0, to_end).start()

        @pl.when(j == LEAD + PIECES - 1)
        def _():
            for early in range(LEAD):
                gather(far_mid, early, 0, to_end).start()

    def inner_end(q):
        gather(end, q, 0, to_end).wait_recv()
        share(end, q).start()
        gather(end, q, 1, to_far).start()

        @pl.when(q == PIECES - 1)
        def _():
            for late in range(LEAD, PIECES):
                gather(z, late, 1, to_far, own).start()

    def pick(table_rows, e):
        lane = lax.broadcasted_iota(jnp.int32, table_rows.shape, 0)
        return jnp.sum(jnp.where(lane == e, table_rows, 0.0), axis=0, keepdims=True)

    def selection(b, e):
        weights = wt[b]
        chosen = jnp.where(weights > 0.0, 1.0, 0.0)
        above = lax.broadcasted_iota(jnp.int32, (rows, rows), 0)
        along = lax.broadcasted_iota(jnp.int32, (rows, rows), 1)
        before = jnp.where(above < along, 1.0, 0.0).astype(bf16)
        rank = jnp.dot(chosen.astype(bf16), before, preferred_element_type=f32)
        place = pick(jnp.where(chosen > 0.0, rank, -1.0), e)
        slot = lax.broadcasted_iota(jnp.int32, (cap, rows), 0).astype(f32)
        return jnp.where(slot == place, 1.0, 0.0), pick(weights, e)

    def hidden_half(first, second, s):
        both = []
        for w in (wg, wu):
            both.append(
                jnp.dot(first, w[s, :half], preferred_element_type=f32)
                + jnp.dot(second, w[s, half:], preferred_element_type=f32)
            )
        gate, upper = both
        return (gate * (0.5 * (1.0 + jnp.tanh(0.5 * gate))) * upper).astype(bf16)

    def lowered(left, right, s):
        return jnp.dot(left, wd[s, :wide], preferred_element_type=f32) + jnp.dot(
            right, wd[s, wide:], preferred_element_type=f32
        )

    def pick_rows(s):
        mark, _ = selection(mid, end * COLS + (y if s == 0 else 1 - y))
        picked[s, c] = jnp.dot(mark.astype(bf16), xn[mid, c], preferred_element_type=f32).astype(bf16)
        chosen_rows(s, to_end).start()

    def got_rows(s):
        chosen_rows(s, to_mid).wait_recv()
        match(s, c).start()

    def slim_first(s):
        match(s, 1 - c).wait_recv()
        slim_hid[s, c] = hidden_half(picked[s, 0], picked[s, 1], s)
        hand_few(s, c).start()

    def slim_weight(s):
        mark, weight_row = selection(mid, end * COLS + (y if s == 0 else 1 - y))
        return jnp.sum(mark * weight_row, axis=1, keepdims=True)

    def slim_rows():
        slim_first(0)
        weight = slim_weight(0)
        hand_few(0, 1 - c).wait_recv()
        slim[0] = (lowered(slim_hid[0, 0], slim_hid[0, 1], 0) * weight).astype(bf16)
        compact(0, to_mid).start()

    def columns_at(k, portion):
        return pl.ds(pl.multiple_of((portion * (CUTS // 2) + k) * columns_cut, columns_cut), columns_cut)

    def slim_columns(at):
        got = jnp.dot(slim_hid[1, 0], wd[1, :wide, at], preferred_element_type=f32) + jnp.dot(
            slim_hid[1, 1], wd[1, wide:, at], preferred_element_type=f32
        )
        slim[1, :, at] = (got * slim_w[...]).astype(bf16)

    def widen(s):
        mark, _ = selection(mid, end * COLS + (y if s == 0 else 1 - y))
        ones = mark.astype(bf16)
        return lax.dot_general(ones, slim_in[s], (((0,), (0,)), ((), ())), preferred_element_type=f32)

    def block_of(k):
        return jnp.where(k == 0, far_end, jnp.where(k == 1, end, jnp.where(k == 2, far_mid, mid)))

    def first_stage(code):
        pair, s = code // 2, code % 2
        b, part_of = block_of(pair // UNITS), pair % UNITS

        @pl.when((s == 0) & (b != z))
        def _():
            shared(b, part_of)
            at = rows_of(part_of)
            normed(b, at, x[b, 0, at], x[b, 1, at])

        at = rows_of(part_of)
        hid[code, c] = hidden_half(xn[b, 0, at], xn[b, 1, at], s)
        hand(pair, s).start()

    def second_stage(pair):
        b, part_of = block_of(pair // UNITS), pair % UNITS
        at = rows_of(part_of)
        mine = columns[b, at]
        lane = lax.broadcasted_iota(jnp.int32, mine.shape, 1)
        both = hid.at[pl.ds(2 * pair, 2), 1 - c]
        remote(both, both, hid_s, hid_r.at[pair], mate).wait_recv()
        sums = None
        for s in range(2):
            expert = z * COLS + (y if s == 0 else 1 - y)
            weight = jnp.sum(jnp.where(lane == expert, mine, 0.0), axis=1, keepdims=True)
            got = lowered(hid[2 * pair + s, 0], hid[2 * pair + s, 1], s) * weight
            sums = got if sums is None else sums + got

        @pl.when(b == z)
        def _():
            acc[at] = sums

        @pl.when(b != z)
        def _():
            part[b, at] = sums.astype(bf16)

        @pl.when(outer & (b != z))
        def _():
            for n in range(per_unit * SPLIT):
                total(b, part_of * per_unit * SPLIT + n, to_mid).start()

    def pass_on(b, q, dev):
        for v in range(SPLIT):
            r = q * SPLIT + v
            total(b, r, dev).wait_recv()
            at = thin(r)
            part[b, at] = (part[b, at].astype(f32) + came[b, at].astype(f32)).astype(bf16)
            total(b, r, dev).start()

    def take_in(q):
        for v in range(SPLIT):
            r = q * SPLIT + v
            total(z, r, to_far).wait_recv()
            at = thin(r)
            acc[at] = acc[at] + came[z, at].astype(f32)

    def look(n, entries):
        value = 0
        for at, entry in entries.items():
            value = jnp.where(n == at, entry, value)
        return value

    head = 3 * CUTS // 2
    outer_first = {
        0: ((1, 0, 0), (1, 1, 0)), 1: ((1, 2, 0), (1, 3, 0)), 10: ((0, 0, 0), (0, 0, 1)), 11: ((0, 1, 0), (0, 1, 1)),
        13: ((0, 2, 0), (0, 2, 1)), 14: ((1, 0, 1), (1, 1, 1)), 15: ((0, 3, 0), (0, 3, 1)), 16: ((1, 2, 1), (1, 3, 1)),
        19: ((2, 0, 0), (2, 0, 1)), 21: ((2, 1, 0), (2, 1, 1)), 23: ((2, 2, 0), (2, 2, 1)), 25: ((2, 3, 0), (2, 3, 1)),
    }
    outer_second = {
        12: ((0, 0), (0, 1)), 13: ((0, 2),), 15: ((0, 3),), 16: ((1, 0), (1, 1)), 17: ((1, 2), (1, 3)),
        19: ((2, 0),), 21: ((2, 1),), 23: ((2, 2),), 25: ((2, 3),),
    }
    outer_pairs = {13: 5, 15: 7, 18: 9, 20: 11, 22: 13, 24: 15}
    inner_first = {
        0: ((3, 0, 0), (3, 1, 0)), 1: ((3, 2, 0), (3, 3, 0)), 2: ((1, 0, 0),), 3: ((2, 0, 0),),
        4: ((1, 1, 0), (0, 0, 0)), 6: ((1, 2, 0), (0, 1, 0)), 8: ((1, 3, 0), (0, 2, 0)),
        9: ((0, 0, 1), (0, 1, 1)), 11: ((0, 3, 0), (0, 2, 1), (0, 3, 1)),
        14: ((1, 0, 1), (1, 1, 1)), 15: ((1, 2, 1), (1, 3, 1)), 16: ((2, 0, 1), (2, 1, 0)), 17: ((2, 1, 1), (2, 2, 0)),
        18: ((2, 2, 1), (2, 3, 0)), 19: ((2, 3, 1), (3, 0, 1)), 20: ((3, 1, 1), (3, 2, 1)), 21: ((3, 3, 1),),
    }
    inner_second = {
        12: ((0, 0), (0, 1)), 13: ((0, 2), (0, 3)), 15: ((1, 0), (1, 1)), 16: ((1, 2), (1, 3)), 17: ((2, 0),),
        18: ((2, 1),), 19: ((2, 2),), 20: ((2, 3), (3, 0)), 21: ((3, 1), (3, 2)), 22: ((3, 3),),
    }

    def packed(plan, width):
        entries = {}
        for at, todo in plan.items():
            entries[at] = 0
            for k, (blk, part_of, *s) in enumerate(todo):
                number = blk * UNITS + part_of
                entries[at] += ((2 * number + s[0] if s else number) + 1) * width ** k
        return entries

    first_width, second_width = 8 * UNITS * 2, 8 * UNITS
    plans = (
        packed(outer_first, first_width), packed(inner_first, first_width),
        packed(outer_second, second_width), packed(inner_second, second_width),
    )

    @pl.when(outer)
    def _():
        table(mid, 0, to_mid).wait_recv()

    @pl.when(inner)
    def _():
        for s in range(2):
            pick_rows(s)
        table(end, 0, to_end).wait_recv()
        table(end, 1, to_far).start()
        table(far_mid, 1, to_far).wait_recv()
        table(far_mid, 0, to_end).start()
        for b in (end, far_mid):
            columns[b] = wt[b].T

    def step(n, carry):
        @pl.when(n < head)
        def _():
            got_y(n)

        ahead = look(n, outer_pairs)

        @pl.when(outer)
        def _():
            @pl.when(n == PIECES // 2)
            def _():
                got_rows(0)
                slim_rows()

            @pl.when(n == PIECES - 1)
            def _():
                got_rows(1)
                slim_w[...] = jnp.broadcast_to(slim_weight(1), slim_w.shape)

            @pl.when((n >= PIECES) & (n < head))
            def _():
                outer_stream(n - PIECES)

            @pl.when(ahead > 0)
            def _():
                outer_stream(ahead - 1)
                outer_stream(ahead)

        @pl.when(inner)
        def _():
            @pl.when(n < PIECES)
            def _():
                inner_end(n)

            @pl.when((n < head) | ((n >= head + 2) & (n < head + 6)))
            def _():
                inner_stream(jnp.where(n < head, n, n - 2))

            @pl.when(n == LEAD)
            def _():
                table(far_end, 1, to_far).wait_recv()
                table(far_end, 0, to_end).start()
                columns[far_end] = wt[far_end].T

        @pl.when(n == PIECES + 1)
        def _():
            got_x(0)
            got_x(1)

        @pl.when(outer)
        def _():
            @pl.when(n == PIECES + 1)
            def _():
                slim_first(1)

            for k in range(CUTS // 2):
                @pl.when(n == min(head, PIECES + 2 + k))
                def _():
                    if k == 0:
                        hand_few(1, 1 - c).wait_recv()
                    for early in ((0, 1), (2,), (), ())[k]:
                        at = columns_at(early, g)
                        slim_columns(at)
                        compact_columns(at).start()
                    got_columns(k)
                    if k < 2:
                        at = columns_at(k, 1 - g)
                        slim_columns(at)
                        compact_columns(at).start()

            @pl.when(n == head + 2)
            def _():
                for k, portion in ((3, g), (2, 1 - g), (3, 1 - g)):
                    slim_columns(columns_at(k, portion))

        @pl.when(outer)
        def _():
            @pl.when(n == head - 1)
            def _():
                table(far_end, 0, to_mid).wait_recv()
                table(far_mid, 0, to_mid).wait_recv()
                for b in (far_end, far_mid):
                    columns[b] = wt[b].T

        @pl.when(inner)
        def _():
            q = n - head - 2

            @pl.when((q >= 0) & (q < PIECES))
            def _():
                pass_on(far_end, q, to_far)

            @pl.when((q >= 3) & (q < PIECES + 3))
            def _():
                pass_on(end, q - 3, to_end)

            @pl.when((q >= PIECES) & (q < 2 * PIECES))
            def _():
                pass_on(far_mid, q - PIECES, to_far)

            @pl.when(q == PIECES + 1)
            def _():
                compact(0, to_end).wait_recv()
                acc[...] = acc[...] + widen(0)

            @pl.when(n == 4 * PIECES - 1)
            def _():
                compact(1, to_end).wait_recv()
                acc[...] = acc[...] + widen(1)

            @pl.when(q >= PIECES + 2)
            def _():
                take_in(q - PIECES - 2)

        todo = jnp.where(outer, look(n, plans[0]), look(n, plans[1]))

        def first(v, left):
            code = left % first_width

            @pl.when(code > 0)
            def _():
                first_stage(code - 1)
            return left // first_width

        lax.fori_loop(0, 4, first, todo)

        @pl.when(inner & (n == head))
        def _():
            for k in range(CUTS // 2):
                got_columns(k)

        todo = jnp.where(outer, look(n, plans[2]), look(n, plans[3]))

        def second(v, left):
            pair = left % second_width

            @pl.when(pair > 0)
            def _():
                second_stage(pair - 1)
            return left // second_width

        lax.fori_loop(0, 2, second, todo)

        @pl.when(outer & (n == 3 * PIECES + 2))
        def _():
            for k, portion in ((3, g), (2, 1 - g), (3, 1 - g)):
                compact_columns(columns_at(k, portion)).start()
        return carry

    lax.fori_loop(0, 4 * PIECES, step, 0)

    @pl.when(outer)
    def _():
        def close(r, carry):
            total(z, r, to_mid).wait_recv()
            at = thin(r)
            out_ref[at] = (acc[at] + came[z, at].astype(f32)).astype(bf16)
            return carry

        lax.fori_loop(0, PIECES * SPLIT, close, 0)

    @pl.when(inner)
    def _():
        out_ref[...] = acc[...].astype(bf16)

    swap(0, PIECES).wait_send()
    send_extra().wait_send()
    for m in range(3):
        send_y(m, 0, CUTS).wait_send()
        send_x(m, 0, g, CUTS if m < 2 else CUTS - 2).wait_send()

    def handed(count):
        at = hid.at[pl.ds(0, count), c]
        remote(at, at, hid_s, hid_r.at[0], mate).wait_send()

    def blocks_shared(blocks):
        for b in blocks:
            remote(x.at[b, c], x.at[b, c], half_s.at[b], half_r.at[b, 0], mate).wait_send()

    @pl.when(outer)
    def _():
        table(z, 0, to_mid).wait_send()
        remote(slim, slim_in, slim_s, slim_r.at[0], to_mid).wait_send()
        at = slim_hid.at[pl.ds(0, 2), c]
        remote(at, at, few_s, few_r.at[0], mate).wait_send()
        handed(6 * UNITS)
        at = picked.at[pl.ds(0, 2), c]
        remote(at, at, match_s, match_r.at[0], mate).wait_send()
        gather_sent(z, 0, to_mid)
        for b in (far_end, far_mid):
            total_sent(b, to_mid)
        blocks_shared((far_end, far_mid))

    @pl.when(inner)
    def _():
        handed(8 * UNITS)
        table(z, 0, to_end).wait_send()
        table(z, 1, to_far).wait_send()
        table(end, 1, to_far).wait_send()
        table(far_mid, 0, to_end).wait_send()
        table(far_end, 0, to_end).wait_send()
        at = picked.at[pl.ds(0, 2), c]
        remote(at, at, pick_s, pick_r.at[0], to_end).wait_send()
        for b in (far_mid, far_end):
            gather_sent(b, 0, to_end)
        for b in (z, end):
            gather_sent(b, 1, to_far)
        total_sent(end, to_end)
        for b in (far_mid, far_end):
            total_sent(b, to_far)
        blocks_shared((end, far_mid, far_end))


def line_form(tokens, norm_gain, expert_ids, route_weights, gate_weight, up_weight, down_weight):
    tok_rows, half = tokens.shape
    experts = lax.axis_size("ep")
    length = experts // COLS
    top = expert_ids.shape[1]
    cap = (3 * tok_rows * top + 2 * experts - 1) // (2 * experts)
    bf16, f32 = jnp.bfloat16, jnp.float32
    gate, up, down = gate_weight[0], up_weight[0], down_weight[0]
    dma, vmem = pltpu.SemaphoreType.DMA, pltpu.VMEM
    block = (length, tok_rows, half)
    pairs = UNITS * length
    bits = (length, PIECES)
    sems = [dma, dma((PIECES,)), dma((7,))]
    for send, recv in (
        ((4,), (3, CUTS)), ((3,), (2 + CUTS // 2,)), ((2, length), bits), ((2, length), (length,)),
        ((length,), (length, UNITS)), ((), (pairs,)), ((), (2,)), ((), (2,)), ((), (2,)), ((length,), (length, PIECES * SPLIT)), ((), (2,)),
    ):
        sems += [dma(send) if send else dma, dma(recv)]
    return pl.pallas_call(
        functools.partial(line_kernel, length, cap),
        out_shape=vmem((tok_rows, half), bf16),
        in_specs=[pl.BlockSpec(memory_space=pl.ANY)] * 7,
        out_specs=pl.BlockSpec(memory_space=vmem),
        scratch_shapes=[
            vmem((tok_rows, half), bf16),
            vmem((2, 1, half), f32),
            vmem((top, tok_rows), jnp.int32),
            vmem((top, tok_rows), f32),
            vmem((tok_rows, half), bf16),
            vmem((length, 2, tok_rows, half), bf16),
            vmem((length, 2, tok_rows, half), bf16),
            vmem((length, experts, tok_rows), f32),
            vmem((length, tok_rows, experts), f32),
            vmem((2,) + gate.shape, bf16),
            vmem((2,) + up.shape, bf16),
            vmem((2,) + down.shape, bf16),
            vmem((2 * pairs, 2, tok_rows // UNITS, gate.shape[1]), bf16),
            vmem((2, 2, cap, gate.shape[1]), bf16),
            vmem((2, 2, cap, half), bf16),
            vmem((cap, half // CUTS), f32),
            vmem(block, bf16),
            vmem(block, bf16),
            vmem((2, cap, half), bf16),
            vmem((2, cap, half), bf16),
            vmem((tok_rows, half), f32),
        ]
        + sems,
        compiler_params=pltpu.CompilerParams(
            collective_id=0, has_side_effects=True, vmem_limit_bytes=58 * 1024 * 1024
        ),
    )(tokens, norm_gain.reshape(2, 1, half), expert_ids.T, route_weights.T, gate, up, down)


def solution(mesh):
    in_specs = (
        P(("grp", "ep"), "tp"),
        P(),
        P(("grp", "ep"), None),
        P(("grp", "ep"), None),
        P("ep", None, "tp"),
        P("ep", None, "tp"),
        P("ep", None, "tp"),
    )
    out_specs = P(("grp", "ep"), "tp")
    shape = mesh.shape

    def on_device(tokens, norm_gain, expert_ids, *rest):
        dense = shape["ep"] == 4 * COLS and shape["ep"] == 4 * expert_ids.shape[1]
        form = line_form if dense and shape["grp"] == 2 and shape["tp"] == 2 else sparse_form
        return form(tokens, norm_gain, expert_ids, *rest)

    return jax.shard_map(
        on_device, mesh=mesh, in_specs=in_specs, out_specs=out_specs, check_vma=False
    )
```

```python
import functools

import jax
import jax.numpy as jnp
from jax import lax
from jax.experimental import pallas as pl
from jax.experimental.pallas import tpu as pltpu
from jax.sharding import PartitionSpec as P

MESH = pl.DeviceIdType.MESH
COLS = 2
PIECES = 8
UNITS = 4
LEAD = 2
SPLIT = 2
CUTS = 8


def normalize(rows, norm_gain):
    xf = rows.astype(jnp.float32)
    scale = lax.rsqrt(jnp.mean(xf * xf, axis=-1, keepdims=True) + 1e-06)
    return (xf * scale * norm_gain[None, :]).astype(jnp.bfloat16)


def sparse_form(tokens, norm_gain, expert_ids, route_weights, gate_weight, up_weight, down_weight):
    tok_rows, half = tokens.shape
    width = half * lax.axis_size("tp")
    experts = lax.axis_size("ep")
    top = expert_ids.shape[1]
    capacity = max(2, (3 * tok_rows * top + 2 * experts - 1) // (2 * experts))
    flat = expert_ids.reshape(-1)
    onehot = (flat[:, None] == jnp.arange(experts, dtype=jnp.int32)[None, :]).astype(jnp.int32)
    earlier = jnp.cumsum(onehot, axis=0) - onehot
    slot = jnp.sum(earlier * onehot, axis=-1)
    position = flat * capacity + slot
    owner = jnp.arange(flat.shape[0], dtype=jnp.int32) // top
    w_gate = gate_weight[0]
    w_up = up_weight[0]
    w_down = down_weight[0]
    send = jnp.zeros((experts * capacity, half), jnp.bfloat16).at[position].set(tokens[owner])
    send = send.reshape(experts, capacity, half)
    received = lax.all_to_all(send, "ep", split_axis=0, concat_axis=0, tiled=True)
    sources = received.shape[0]
    count = received.shape[1]
    whole_rows = lax.all_gather(received, "tp", axis=2, tiled=True)
    rows = normalize(whole_rows.reshape(sources * count, width), norm_gain)
    gate = jnp.dot(rows, w_gate, preferred_element_type=jnp.float32)
    upper = jnp.dot(rows, w_up, preferred_element_type=jnp.float32)
    hidden = (jax.nn.silu(gate) * upper).astype(jnp.bfloat16)
    result = jnp.dot(
        lax.all_gather(hidden, "tp", axis=1, tiled=True), w_down, preferred_element_type=jnp.float32
    )
    result = result.astype(jnp.bfloat16).reshape(sources, count, half)
    back = lax.all_to_all(result, "ep", split_axis=0, concat_axis=0, tiled=True)
    picked = back.reshape(experts * capacity, half)[position].astype(jnp.float32)
    picked = picked * route_weights.reshape(-1)[:, None]
    return jnp.sum(picked.reshape(tok_rows, top, half), axis=1).astype(jnp.bfloat16)


def line_kernel(
    length, cap, tok_ref, gain_in, ids_in, route_in, gate_in, up_in, down_in, out_ref,
    own, gain_ref, ids_ref, route_ref, raw, x, xn, wt, columns, wg, wu, wd, hid, slim_hid, picked, slim_w, part, came, slim, slim_in, acc,
    swap_s, swap_r, loc, wy_s, wy_r, wx_s, wx_r, gat_s, gat_r, tab_s, tab_r,
    half_s, half_r, hid_s, hid_r, few_s, few_r, pick_s, pick_r, match_s, match_r, sum_s, sum_r, slim_s, slim_r,
):
    f32, bf16 = jnp.float32, jnp.bfloat16
    g, ep, c = lax.axis_index("grp"), lax.axis_index("ep"), lax.axis_index("tp")
    z, y = ep // COLS, ep % COLS
    last = length - 1
    flip = z >= length // 2
    end = jnp.where(flip, last, 0)
    mid = jnp.where(flip, last - 1, 1)
    far_mid, far_end = last - mid, last - end
    outer, inner = z == end, z == mid
    mate, across, beside = {"tp": 1 - c}, {"grp": 1 - g}, {"ep": z * COLS + 1 - y}
    to_end, to_mid, to_far = {"ep": end * COLS + y}, {"ep": mid * COLS + y}, {"ep": far_mid * COLS + y}
    rows, half = raw.shape
    piece = rows // PIECES
    unit = rows // UNITS
    per_unit = PIECES // UNITS
    wide = hid.shape[3]

    def remote(src, dst, ss, rs, dev):
        return pltpu.make_async_remote_copy(
            src_ref=src, dst_ref=dst, send_sem=ss, recv_sem=rs, device_id=dev, device_id_type=MESH
        )

    def span(q):
        return pl.ds(q * piece if isinstance(q, int) else pl.multiple_of(q * piece, piece), piece)

    barrier = pltpu.get_barrier_semaphore()
    for dev in (mate, across, beside):
        pl.semaphore_signal(barrier, inc=1, device_id=dev, device_id_type=MESH)

    @pl.when(outer)
    def _():
        pl.semaphore_signal(barrier, inc=1, device_id=to_mid, device_id_type=MESH)

    @pl.when(inner)
    def _():
        pl.semaphore_signal(barrier, inc=1, device_id=to_end, device_id_type=MESH)
        pl.semaphore_signal(barrier, inc=1, device_id=to_far, device_id_type=MESH)

    inputs = ((tok_ref, own), (gain_in, gain_ref), (ids_in, ids_ref), (route_in, route_ref))
    inputs += ((gate_in, wg.at[0]), (up_in, wu.at[0]), (down_in, wd.at[0]))
    local = [pltpu.make_async_copy(src, dst, loc.at[k]) for k, (src, dst) in enumerate(inputs)]
    for copy in local:
        copy.start()
    pl.semaphore_wait(barrier, jnp.where(outer, 4, 5))

    mats = ((gate_in, wg), (up_in, wu), (down_in, wd))

    columns_cut = down_in.shape[1] // CUTS

    def cut(m, portion, u, many=1):
        if m < 2:
            size = mats[m][0].shape[0] // (2 * CUTS)
            return (pl.ds(pl.multiple_of((portion * CUTS + u) * size, size), size * many), pl.ds(0, wide))
        first = pl.multiple_of((portion * (CUTS // 2) + u // 2) * columns_cut, columns_cut)
        if many == 1:
            return (pl.ds(pl.multiple_of(u % 2 * wide, wide), wide), pl.ds(first, columns_cut))
        return (pl.ds(0, 2 * wide), pl.ds(first, columns_cut * (many // 2)))

    def send_y(m, u, many=1):
        dst = mats[m][1]
        at = cut(m, g, u, many)
        return remote(dst.at[(0,) + at], dst.at[(1,) + at], wy_s.at[m], wy_r.at[m, u], beside)

    def send_extra():
        at = cut(2, 1 - g, CUTS - 2, 2)
        return remote(
            wd.at[(0,) + at], wd.at[(1,) + at], wy_s.at[3], wx_r.at[1 + CUTS // 2], beside
        )

    def send_x(m, u, portion, many=1):
        buf = mats[m][1].at[(1,) + cut(m, portion, u, many)]
        return remote(buf, buf, wx_s.at[m], wx_r.at[m if m < 2 else 2 + u // 2], across)

    def swap(q, many=1):
        at = pl.ds(q * piece if isinstance(q, int) else pl.multiple_of(q * piece, piece), piece * many)
        return remote(own.at[at], raw.at[at], swap_s, swap_r.at[q], mate)

    def gather(b, q, way, dev, src=None):
        at = x.at[b, c, span(q)]
        return remote(at if src is None else src.at[span(q)], at, gat_s.at[way, b], gat_r.at[b, q], dev)

    for copy in local[2:4]:
        copy.wait()
    def table(b, way, dev):
        return remote(wt.at[b], wt.at[b], tab_s.at[way, b], tab_r.at[b], dev)

    named = lax.broadcasted_iota(jnp.int32, wt.shape[1:], 0)
    routes = None
    for k in range(ids_ref.shape[0]):
        term = jnp.where(named == ids_ref[pl.ds(k, 1)], route_ref[pl.ds(k, 1)], 0.0)
        routes = term if routes is None else routes + term
    wt[z] = routes

    @pl.when(outer)
    def _():
        table(z, 0, to_mid).start()

    @pl.when(inner)
    def _():
        table(z, 0, to_end).start()
        table(z, 1, to_far).start()

    local[0].wait()

    @pl.when(outer)
    def _():
        for q in range(PIECES):
            gather(z, q, 0, to_mid, own).start()

    @pl.when(inner)
    def _():
        for q in range(LEAD):
            gather(z, q, 1, to_far, own).start()

    for q in range(PIECES):
        swap(q).start()
    for m in range(3):
        local[4 + m].wait()
        for u in range(CUTS):
            send_y(m, u).start()
    send_extra().start()
    local[1].wait()

    def gather_sent(b, way, dev):
        remote(x.at[b, c], x.at[b, c], gat_s.at[way, b], gat_r.at[b, 0], dev).wait_send()

    def share(b, q):
        at = x.at[b, c, span(q)]
        return remote(at, at, half_s.at[b], half_r.at[b, q // per_unit], mate)

    def shared(b, part_of):
        at = x.at[b, 1 - c, rows_of(part_of)]
        remote(at, at, half_s.at[b], half_r.at[b, part_of], mate).wait_recv()

    def rows_of(part_of):
        return pl.ds(part_of * unit if isinstance(part_of, int) else pl.multiple_of(part_of * unit, unit), unit)

    def thin(r):
        size = piece // SPLIT
        return pl.ds(r * size if isinstance(r, int) else pl.multiple_of(r * size, size), size)

    def total(b, q, dev):
        return remote(part.at[b, thin(q)], came.at[b, thin(q)], sum_s.at[b], sum_r.at[b, q], dev)

    def total_sent(b, dev):
        remote(part.at[b], came.at[b], sum_s.at[b], sum_r.at[b, 0], dev).wait_send()

    def compact(s, dev):
        return remote(slim.at[s], slim_in.at[s], slim_s, slim_r.at[s], dev)

    def hand(pair, s):
        at = hid.at[2 * pair + s, c]
        return remote(at, at, hid_s, hid_r.at[pair], mate)

    def chosen_rows(s, dev):
        at = picked.at[s, c]
        return remote(at, at, pick_s, pick_r.at[s], dev)

    def match(s, side):
        at = picked.at[s, side]
        return remote(at, at, match_s, match_r.at[s], mate)

    def compact_columns(at):
        return remote(slim.at[1, :, at], slim_in.at[1, :, at], slim_s, slim_r.at[1], to_mid)

    def hand_few(s, side):
        at = slim_hid.at[s, side]
        return remote(at, at, few_s, few_r.at[s], mate)

    def normed(b, at, first, second):
        a, d = first.astype(f32), second.astype(f32)
        squares = jnp.sum(a * a, axis=-1, keepdims=True) + jnp.sum(d * d, axis=-1, keepdims=True)
        scale = lax.rsqrt(squares / (2 * half) + 1e-06)
        xn[b, 0, at] = (a * scale * gain_ref[0]).astype(bf16)
        xn[b, 1, at] = (d * scale * gain_ref[1]).astype(bf16)

    def norm(q, carry):
        swap(q).wait_recv()
        at = span(q)
        mine, other = own[at], raw[at]
        normed(z, at, jnp.where(c == 0, mine, other), jnp.where(c == 0, other, mine))
        return carry

    lax.fori_loop(0, PIECES, norm, 0)
    columns[z] = wt[z].T

    def got_y(n):
        for m in range(3):
            @pl.when(n // (CUTS // 2) == m)
            def _():
                for v in range(2):
                    u = n % (CUTS // 2) * 2 + v
                    send_y(m, u).wait_recv()

                    @pl.when((m < 2) | (u < CUTS - 2))
                    def _():
                        send_x(m, u, g).start()

    def got_x(m):
        send_x(m, 0, 1 - g, CUTS).wait_recv()

    def got_columns(k):
        if k == CUTS // 2 - 1:
            send_extra().wait_recv()
        else:
            send_x(2, 2 * k, 1 - g, 2).wait_recv()

    def outer_stream(j):
        b = jnp.where(j < PIECES, far_end, far_mid)
        q = j % PIECES
        gather(b, q, 0, to_mid).wait_recv()
        share(b, q).start()

    def inner_stream(j):
        lead = j < LEAD
        turn = (j >= LEAD) & (j < LEAD + PIECES)
        b = jnp.where(turn, far_end, far_mid)
        q = jnp.where(lead, j, jnp.where(turn, j - LEAD, j - PIECES))
        gather(b, q, 1, to_far).wait_recv()
        share(b, q).start()

        @pl.when(j >= LEAD)
        def _():
            gather(b, q, 0, to_end).start()

        @pl.when(j == LEAD + PIECES - 1)
        def _():
            for early in range(LEAD):
                gather(far_mid, early, 0, to_end).start()

    def inner_end(q):
        gather(end, q, 0, to_end).wait_recv()
        share(end, q).start()
        gather(end, q, 1, to_far).start()

        @pl.when(q == PIECES - 1)
        def _():
            for late in range(LEAD, PIECES):
                gather(z, late, 1, to_far, own).start()

    def pick(table_rows, e):
        lane = lax.broadcasted_iota(jnp.int32, table_rows.shape, 0)
        return jnp.sum(jnp.where(lane == e, table_rows, 0.0), axis=0, keepdims=True)

    def selection(b, e):
        weights = wt[b]
        chosen = jnp.where(weights > 0.0, 1.0, 0.0)
        above = lax.broadcasted_iota(jnp.int32, (rows, rows), 0)
        along = lax.broadcasted_iota(jnp.int32, (rows, rows), 1)
        before = jnp.where(above < along, 1.0, 0.0).astype(bf16)
        rank = jnp.dot(chosen.astype(bf16), before, preferred_element_type=f32)
        place = pick(jnp.where(chosen > 0.0, rank, -1.0), e)
        slot = lax.broadcasted_iota(jnp.int32, (cap, rows), 0).astype(f32)
        return jnp.where(slot == place, 1.0, 0.0), pick(weights, e)

    def hidden_half(first, second, s):
        both = []
        for w in (wg, wu):
            both.append(
                jnp.dot(first, w[s, :half], preferred_element_type=f32)
                + jnp.dot(second, w[s, half:], preferred_element_type=f32)
            )
        gate, upper = both
        return (gate * (0.5 * (1.0 + jnp.tanh(0.5 * gate))) * upper).astype(bf16)

    def lowered(left, right, s):
        return jnp.dot(left, wd[s, :wide], preferred_element_type=f32) + jnp.dot(
            right, wd[s, wide:], preferred_element_type=f32
        )

    def pick_rows(s):
        mark, _ = selection(mid, end * COLS + (y if s == 0 else 1 - y))
        picked[s, c] = jnp.dot(mark.astype(bf16), xn[mid, c], preferred_element_type=f32).astype(bf16)
        chosen_rows(s, to_end).start()

    def got_rows(s):
        chosen_rows(s, to_mid).wait_recv()
        match(s, c).start()

    def slim_first(s):
        match(s, 1 - c).wait_recv()
        slim_hid[s, c] = hidden_half(picked[s, 0], picked[s, 1], s)
        hand_few(s, c).start()

    def slim_weight(s):
        mark, weight_row = selection(mid, end * COLS + (y if s == 0 else 1 - y))
        return jnp.sum(mark * weight_row, axis=1, keepdims=True)

    def slim_rows():
        slim_first(0)
        weight = slim_weight(0)
        hand_few(0, 1 - c).wait_recv()
        slim[0] = (lowered(slim_hid[0, 0], slim_hid[0, 1], 0) * weight).astype(bf16)
        compact(0, to_mid).start()

    def columns_at(k, portion):
        return pl.ds(pl.multiple_of((portion * (CUTS // 2) + k) * columns_cut, columns_cut), columns_cut)

    def slim_columns(at):
        got = jnp.dot(slim_hid[1, 0], wd[1, :wide, at], preferred_element_type=f32) + jnp.dot(
            slim_hid[1, 1], wd[1, wide:, at], preferred_element_type=f32
        )
        slim[1, :, at] = (got * slim_w[...]).astype(bf16)

    def widen(s):
        mark, _ = selection(mid, end * COLS + (y if s == 0 else 1 - y))
        ones = mark.astype(bf16)
        return lax.dot_general(ones, slim_in[s], (((0,), (0,)), ((), ())), preferred_element_type=f32)

    def block_of(k):
        return jnp.where(k == 0, far_end, jnp.where(k == 1, end, jnp.where(k == 2, far_mid, mid)))

    def first_stage(code):
        pair, s = code // 2, code % 2
        b, part_of = block_of(pair // UNITS), pair % UNITS

        @pl.when((s == 0) & (b != z))
        def _():
            shared(b, part_of)
            at = rows_of(part_of)
            normed(b, at, x[b, 0, at], x[b, 1, at])

        at = rows_of(part_of)
        hid[code, c] = hidden_half(xn[b, 0, at], xn[b, 1, at], s)
        hand(pair, s).start()

    def second_stage(pair):
        b, part_of = block_of(pair // UNITS), pair % UNITS
        at = rows_of(part_of)
        mine = columns[b, at]
        lane = lax.broadcasted_iota(jnp.int32, mine.shape, 1)
        both = hid.at[pl.ds(2 * pair, 2), 1 - c]
        remote(both, both, hid_s, hid_r.at[pair], mate).wait_recv()
        sums = None
        for s in range(2):
            expert = z * COLS + (y if s == 0 else 1 - y)
            weight = jnp.sum(jnp.where(lane == expert, mine, 0.0), axis=1, keepdims=True)
            got = lowered(hid[2 * pair + s, 0], hid[2 * pair + s, 1], s) * weight
            sums = got if sums is None else sums + got

        @pl.when(b == z)
        def _():
            acc[at] = sums

        @pl.when(b != z)
        def _():
            part[b, at] = sums.astype(bf16)

        @pl.when(outer & (b != z))
        def _():
            for n in range(per_unit * SPLIT):
                total(b, part_of * per_unit * SPLIT + n, to_mid).start()

    def pass_on(b, q, dev):
        for v in range(SPLIT):
            r = q * SPLIT + v
            total(b, r, dev).wait_recv()
            at = thin(r)
            part[b, at] = (part[b, at].astype(f32) + came[b, at].astype(f32)).astype(bf16)
            total(b, r, dev).start()

    def take_in(q):
        for v in range(SPLIT):
            r = q * SPLIT + v
            total(z, r, to_far).wait_recv()
            at = thin(r)
            acc[at] = acc[at] + came[z, at].astype(f32)

    def look(n, entries):
        value = 0
        for at, entry in entries.items():
            value = jnp.where(n == at, entry, value)
        return value

    head = 3 * CUTS // 2
    outer_first = {
        0: ((1, 0, 0), (1, 1, 0)), 1: ((1, 2, 0), (1, 3, 0)), 10: ((0, 0, 0), (0, 0, 1)), 13: ((0, 1, 0), (0, 1, 1)),
        14: ((0, 2, 0), (0, 2, 1)), 15: ((1, 0, 1), (1, 1, 1)), 16: ((0, 3, 0), (0, 3, 1)), 17: ((1, 2, 1), (1, 3, 1)),
        19: ((2, 0, 0), (2, 0, 1)), 21: ((2, 1, 0), (2, 1, 1)), 23: ((2, 2, 0), (2, 2, 1)), 25: ((2, 3, 0), (2, 3, 1)),
    }
    outer_second = {
        12: ((0, 0),), 13: ((0, 1),), 14: ((0, 2),), 16: ((0, 3),), 17: ((1, 0), (1, 1)), 18: ((1, 2), (1, 3)),
        19: ((2, 0),), 21: ((2, 1),), 23: ((2, 2),), 25: ((2, 3),),
    }
    outer_pairs = {14: 5, 16: 7, 18: 9, 20: 11, 22: 13, 24: 15}
    inner_first = {
        0: ((3, 0, 0), (3, 1, 0)), 1: ((3, 2, 0), (3, 3, 0)), 2: ((1, 0, 0),), 3: ((2, 0, 0),),
        4: ((1, 1, 0), (0, 0, 0)), 6: ((1, 2, 0), (0, 1, 0)), 8: ((1, 3, 0), (0, 2, 0)),
        9: ((0, 0, 1), (0, 1, 1)), 11: ((0, 3, 0), (0, 2, 1), (0, 3, 1)),
        14: ((1, 0, 1), (1, 1, 1)), 15: ((1, 2, 1), (1, 3, 1)), 16: ((2, 0, 1), (2, 1, 0)), 17: ((2, 1, 1), (2, 2, 0)),
        18: ((2, 2, 1), (2, 3, 0)), 19: ((2, 3, 1), (3, 0, 1)), 20: ((3, 1, 1), (3, 2, 1)), 21: ((3, 3, 1),),
    }
    inner_second = {
        12: ((0, 0), (0, 1)), 13: ((0, 2), (0, 3)), 15: ((1, 0), (1, 1)), 16: ((1, 2), (1, 3)), 17: ((2, 0),),
        18: ((2, 1),), 19: ((2, 2),), 20: ((2, 3), (3, 0)), 21: ((3, 1), (3, 2)), 22: ((3, 3),),
    }

    def packed(plan, width):
        entries = {}
        for at, todo in plan.items():
            entries[at] = 0
            for k, (blk, part_of, *s) in enumerate(todo):
                number = blk * UNITS + part_of
                entries[at] += ((2 * number + s[0] if s else number) + 1) * width ** k
        return entries

    first_width, second_width = 8 * UNITS * 2, 8 * UNITS
    plans = (
        packed(outer_first, first_width), packed(inner_first, first_width),
        packed(outer_second, second_width), packed(inner_second, second_width),
    )

    @pl.when(outer)
    def _():
        table(mid, 0, to_mid).wait_recv()

    @pl.when(inner)
    def _():
        for s in range(2):
            pick_rows(s)
        table(end, 0, to_end).wait_recv()
        table(end, 1, to_far).start()
        table(far_mid, 1, to_far).wait_recv()
        table(far_mid, 0, to_end).start()
        for b in (end, far_mid):
            columns[b] = wt[b].T

    def step(n, carry):
        @pl.when(inner & (n < PIECES))
        def _():
            inner_end(n)

        @pl.when(n < head)
        def _():
            got_y(n)

        ahead = look(n, outer_pairs)

        @pl.when(outer)
        def _():
            @pl.when(n == PIECES // 2)
            def _():
                got_rows(0)
                slim_rows()

            @pl.when(n == PIECES - 1)
            def _():
                got_rows(1)
                slim_w[...] = jnp.broadcast_to(slim_weight(1), slim_w.shape)

            @pl.when((n >= PIECES) & (n < head))
            def _():
                outer_stream(n - PIECES)

            @pl.when(ahead > 0)
            def _():
                outer_stream(ahead - 1)
                outer_stream(ahead)

        @pl.when(inner)
        def _():
            @pl.when((n < head) | ((n >= head + 2) & (n < head + 6)))
            def _():
                inner_stream(jnp.where(n < head, n, n - 2))

            @pl.when(n == LEAD)
            def _():
                table(far_end, 1, to_far).wait_recv()
                table(far_end, 0, to_end).start()
                columns[far_end] = wt[far_end].T

        @pl.when(n == PIECES + 1)
        def _():
            got_x(0)
            got_x(1)

        @pl.when(outer)
        def _():
            @pl.when(n == PIECES + 1)
            def _():
                slim_first(1)

            for k in range(CUTS // 2):
                @pl.when(n == min(head, PIECES + 2 + k))
                def _():
                    if k == 0:
                        hand_few(1, 1 - c).wait_recv()
                    for early in ((0, 1), (2,), (), ())[k]:
                        at = columns_at(early, g)
                        slim_columns(at)
                        compact_columns(at).start()
                    got_columns(k)
                    if k < 2:
                        at = columns_at(k, 1 - g)
                        slim_columns(at)
                        compact_columns(at).start()

            @pl.when(n == head + 3)
            def _():
                for k, portion in ((3, g), (2, 1 - g), (3, 1 - g)):
                    slim_columns(columns_at(k, portion))

        @pl.when(outer)
        def _():
            @pl.when(n == head - 1)
            def _():
                table(far_end, 0, to_mid).wait_recv()
                table(far_mid, 0, to_mid).wait_recv()
                for b in (far_end, far_mid):
                    columns[b] = wt[b].T

        @pl.when(inner)
        def _():
            q = n - head - 2

            @pl.when((q >= 0) & (q < PIECES))
            def _():
                pass_on(far_end, q, to_far)

            @pl.when((q >= 3) & (q < PIECES + 3))
            def _():
                pass_on(end, q - 3, to_end)

            @pl.when((q >= PIECES) & (q < 2 * PIECES))
            def _():
                pass_on(far_mid, q - PIECES, to_far)

            @pl.when(q == PIECES + 1)
            def _():
                compact(0, to_end).wait_recv()
                acc[...] = acc[...] + widen(0)

            @pl.when(n == 4 * PIECES - 1)
            def _():
                compact(1, to_end).wait_recv()
                acc[...] = acc[...] + widen(1)
                early = pl.ds(0, rows - piece)
                out_ref[early] = acc[early].astype(bf16)

            @pl.when(q >= PIECES + 2)
            def _():
                take_in(q - PIECES - 2)

        todo = jnp.where(outer, look(n, plans[0]), look(n, plans[1]))

        def first(v, left):
            code = left % first_width

            @pl.when(code > 0)
            def _():
                first_stage(code - 1)
            return left // first_width

        lax.fori_loop(0, 4, first, todo)

        @pl.when(inner & (n == head))
        def _():
            for k in range(CUTS // 2):
                got_columns(k)

        todo = jnp.where(outer, look(n, plans[2]), look(n, plans[3]))

        def second(v, left):
            pair = left % second_width

            @pl.when(pair > 0)
            def _():
                second_stage(pair - 1)
            return left // second_width

        lax.fori_loop(0, 2, second, todo)

        @pl.when(outer & (n == 3 * PIECES + 2))
        def _():
            for k, portion in ((3, g), (2, 1 - g), (3, 1 - g)):
                compact_columns(columns_at(k, portion)).start()
        return carry

    lax.fori_loop(0, 4 * PIECES, step, 0)

    @pl.when(outer)
    def _():
        def close(r, carry):
            total(z, r, to_mid).wait_recv()
            at = thin(r)
            out_ref[at] = (acc[at] + came[z, at].astype(f32)).astype(bf16)
            return carry

        lax.fori_loop(0, PIECES * SPLIT, close, 0)

    @pl.when(inner)
    def _():
        end_rows = pl.ds(rows - piece, piece)
        out_ref[end_rows] = acc[end_rows].astype(bf16)

    swap(0, PIECES).wait_send()
    send_extra().wait_send()
    for m in range(3):
        send_y(m, 0, CUTS).wait_send()
        send_x(m, 0, g, CUTS if m < 2 else CUTS - 2).wait_send()

    def handed(count):
        at = hid.at[pl.ds(0, count), c]
        remote(at, at, hid_s, hid_r.at[0], mate).wait_send()

    def blocks_shared(blocks):
        for b in blocks:
            remote(x.at[b, c], x.at[b, c], half_s.at[b], half_r.at[b, 0], mate).wait_send()

    @pl.when(outer)
    def _():
        table(z, 0, to_mid).wait_send()
        remote(slim, slim_in, slim_s, slim_r.at[0], to_mid).wait_send()
        at = slim_hid.at[pl.ds(0, 2), c]
        remote(at, at, few_s, few_r.at[0], mate).wait_send()
        handed(6 * UNITS)
        at = picked.at[pl.ds(0, 2), c]
        remote(at, at, match_s, match_r.at[0], mate).wait_send()
        gather_sent(z, 0, to_mid)
        for b in (far_end, far_mid):
            total_sent(b, to_mid)
        blocks_shared((far_end, far_mid))

    @pl.when(inner)
    def _():
        handed(8 * UNITS)
        table(z, 0, to_end).wait_send()
        table(z, 1, to_far).wait_send()
        table(end, 1, to_far).wait_send()
        table(far_mid, 0, to_end).wait_send()
        table(far_end, 0, to_end).wait_send()
        at = picked.at[pl.ds(0, 2), c]
        remote(at, at, pick_s, pick_r.at[0], to_end).wait_send()
        for b in (far_mid, far_end):
            gather_sent(b, 0, to_end)
        for b in (z, end):
            gather_sent(b, 1, to_far)
        total_sent(end, to_end)
        for b in (far_mid, far_end):
            total_sent(b, to_far)
        blocks_shared((end, far_mid, far_end))


def line_form(tokens, norm_gain, expert_ids, route_weights, gate_weight, up_weight, down_weight):
    tok_rows, half = tokens.shape
    experts = lax.axis_size("ep")
    length = experts // COLS
    top = expert_ids.shape[1]
    cap = (3 * tok_rows * top + 2 * experts - 1) // (2 * experts)
    bf16, f32 = jnp.bfloat16, jnp.float32
    gate, up, down = gate_weight[0], up_weight[0], down_weight[0]
    dma, vmem = pltpu.SemaphoreType.DMA, pltpu.VMEM
    block = (length, tok_rows, half)
    pairs = UNITS * length
    bits = (length, PIECES)
    sems = [dma, dma((PIECES,)), dma((7,))]
    for send, recv in (
        ((4,), (3, CUTS)), ((3,), (2 + CUTS // 2,)), ((2, length), bits), ((2, length), (length,)),
        ((length,), (length, UNITS)), ((), (pairs,)), ((), (2,)), ((), (2,)), ((), (2,)), ((length,), (length, PIECES * SPLIT)), ((), (2,)),
    ):
        sems += [dma(send) if send else dma, dma(recv)]
    return pl.pallas_call(
        functools.partial(line_kernel, length, cap),
        out_shape=vmem((tok_rows, half), bf16),
        in_specs=[pl.BlockSpec(memory_space=pl.ANY)] * 7,
        out_specs=pl.BlockSpec(memory_space=vmem),
        scratch_shapes=[
            vmem((tok_rows, half), bf16),
            vmem((2, 1, half), f32),
            vmem((top, tok_rows), jnp.int32),
            vmem((top, tok_rows), f32),
            vmem((tok_rows, half), bf16),
            vmem((length, 2, tok_rows, half), bf16),
            vmem((length, 2, tok_rows, half), bf16),
            vmem((length, experts, tok_rows), f32),
            vmem((length, tok_rows, experts), f32),
            vmem((2,) + gate.shape, bf16),
            vmem((2,) + up.shape, bf16),
            vmem((2,) + down.shape, bf16),
            vmem((2 * pairs, 2, tok_rows // UNITS, gate.shape[1]), bf16),
            vmem((2, 2, cap, gate.shape[1]), bf16),
            vmem((2, 2, cap, half), bf16),
            vmem((cap, half // CUTS), f32),
            vmem(block, bf16),
            vmem(block, bf16),
            vmem((2, cap, half), bf16),
            vmem((2, cap, half), bf16),
            vmem((tok_rows, half), f32),
        ]
        + sems,
        compiler_params=pltpu.CompilerParams(
            collective_id=0, has_side_effects=True, vmem_limit_bytes=58 * 1024 * 1024
        ),
    )(tokens, norm_gain.reshape(2, 1, half), expert_ids.T, route_weights.T, gate, up, down)


def solution(mesh):
    in_specs = (
        P(("grp", "ep"), "tp"),
        P(),
        P(("grp", "ep"), None),
        P(("grp", "ep"), None),
        P("ep", None, "tp"),
        P("ep", None, "tp"),
        P("ep", None, "tp"),
    )
    out_specs = P(("grp", "ep"), "tp")
    shape = mesh.shape

    def on_device(tokens, norm_gain, expert_ids, *rest):
        dense = shape["ep"] == 4 * COLS and shape["ep"] == 4 * expert_ids.shape[1]
        form = line_form if dense and shape["grp"] == 2 and shape["tp"] == 2 else sparse_form
        return form(tokens, norm_gain, expert_ids, *rest)

    return jax.shard_map(
        on_device, mesh=mesh, in_specs=in_specs, out_specs=out_specs, check_vma=False
    )
```
